256 devices in a mesh: sp: 32 (over z, x), tp: 8 (over y, core).
Axes of the slice: x: 4, y: 4, z: 8, core: 2. Of those that a mesh axis runs over, the one named last changes fastest.
Arguments:
- residual: bfloat16 [16384, 2048], P('sp'), may hold values from -6 to 6
- queries: bfloat16 [16384, 1024], P('sp', 'tp'), may hold values from -384 to 384
- key_pairs: bfloat16 [16384, 1024], P('sp', 'tp'), may hold values from -384 to 384
- values: bfloat16 [16384, 1024], P('sp', 'tp'), may hold values from -6 to 6
- lambdas: float32 [8], P('tp'), may hold values from 0.3 to 0.8
- head_gain: float32 [128], replicated, may hold values from 0.1 to 1.9
- w_out: bfloat16 [1024, 2048], replicated, may hold values from -0.1875 to 0.1875
- norm_gain: float32 [2048], replicated, may hold values from 0.1 to 1.9
- w_gate: bfloat16 [2048, 5632], P('sp', 'tp'), may hold values from -0.125 to 0.125
- w_up: bfloat16 [2048, 5632], P('sp', 'tp'), may hold values from -0.125 to 0.125
- w_down: bfloat16 [5632, 2048], P('tp', 'sp'), may hold values from -0.078125 to 0.078125
Outputs:
- layer_out: bfloat16 [16384, 2048], P(('sp', 'tp'))
The draws below stay inside these ranges and needn't reach their ends.
All inputs are finite; a program needn't handle non-finite values.
Results may differ from the reference program's by a relative error of at most 0.018.
Values may be sent and summed in bfloat16 or wider, within the bound.
A program may use at most 128 MiB of HBM per device.

```python
import math
import jax
import jax.numpy as jnp
from jax import lax

D = 2048
HEADS = 8
HD = 64
VD = 128
FF = 5632
SEQ = 16384
N_TP = 8


def drawn_pair(key):
    query_key, pair_key = jax.random.split(jax.random.fold_in(key, 11), 2)
    query_draw = jnp.clip(jax.random.normal(query_key, (SEQ, HEADS, 2, HD), jnp.float32), -6.0, 6.0) * 1.3
    key_draw = jnp.clip(jax.random.normal(pair_key, (SEQ, HEADS, 2, HD), jnp.float32), -6.0, 6.0) * 1.3
    return (query_draw.reshape(SEQ, HEADS * 2 * HD), key_draw.reshape(SEQ, HEADS * 2 * HD))


def draw_queries(key, part):
    return drawn_pair(key)[0].astype(jnp.bfloat16)


def draw_key_pairs(key, part):
    return drawn_pair(key)[1].astype(jnp.bfloat16)


def shard_levels(rng, dims, cuts, low, top_value):
    def one(position, blocks):
        draws = jax.random.uniform(jax.random.fold_in(jax.random.fold_in(rng, 6), position), (blocks,), jnp.float32, low / len(cuts), top_value / len(cuts))
        return jnp.repeat(jnp.exp(draws), dims[position] // blocks).reshape((-1,) + (1,) * (len(dims) - position - 1))

    factor_of = one(*cuts[0])
    for cut in cuts[1:]:
        factor_of = factor_of * one(*cut)
    return factor_of


def scatter_about(own_key, shape, deviation, bound, cuts=(), kind=jnp.bfloat16):
    loudness = shard_levels(own_key, shape, cuts, -0.22, 0.18) if cuts else 1.0
    result = jax.random.normal(own_key, shape, jnp.float32) * deviation * loudness
    return jnp.minimum(jnp.maximum(result, -bound), bound).astype(kind)


def setup_inputs(seed: int = 0) -> dict:
    arg_keys = jax.random.split(jax.random.key(seed), 12)
    residual = scatter_about(arg_keys[0], (SEQ, D), 1.0, 6.0, ((0, 32),))
    queries = draw_queries(jax.random.fold_in(arg_keys[11], 71), 0)
    key_pairs = draw_key_pairs(jax.random.fold_in(arg_keys[11], 71), 0)
    values = scatter_about(arg_keys[3], (SEQ, HEADS * VD), 1.0, 6.0, ((0, 32), (1, 8)))
    lambdas = jnp.clip(0.3 + 0.5 * jax.random.uniform(arg_keys[4], (HEADS,), jnp.float32) ** shard_levels(arg_keys[4], (HEADS,), ((0, 8),), -0.2, 0.2), 0.3, 0.8)
    head_gain = jnp.clip(1.0 + 0.18 * jax.random.normal(arg_keys[5], (VD,), jnp.float32), 0.1, 1.9)
    w_out = scatter_about(arg_keys[6], (HEADS * VD, D), (HEADS * VD) ** -0.5, 0.1875)
    norm_gain = jnp.clip(1.0 + 0.18 * jax.random.normal(arg_keys[7], (D,), jnp.float32), 0.1, 1.9)
    w_gate = scatter_about(arg_keys[8], (D, FF), D ** -0.5, 0.125, ((0, 32), (1, 8)))
    w_up = scatter_about(arg_keys[9], (D, FF), D ** -0.5, 0.125, ((0, 32), (1, 8)))
    w_down = scatter_about(arg_keys[10], (FF, D), FF ** -0.5, 0.078125, ((0, 8), (1, 32)))
    return {"residual": residual, "queries": queries, "key_pairs": key_pairs, "values": values, "lambdas": lambdas, "head_gain": head_gain, "w_out": w_out, "norm_gain": norm_gain, "w_gate": w_gate, "w_up": w_up, "w_down": w_down}


def reference(residual, queries, key_pairs, values, lambdas, head_gain, w_out, norm_gain, w_gate, w_up, w_down):
    score_scale = HD ** (-0.5)
    value_width = 2 * HD
    key_all = key_pairs.reshape(SEQ, HEADS, 2, HD).astype(jnp.float32)
    value_all = values.reshape(SEQ, HEADS, value_width).astype(jnp.float32)
    query_rows = math.gcd(SEQ, 256)

    def attend(query_block):
        scores = jnp.einsum('qhmd,khmd->hmqk', query_block.astype(jnp.float32), key_all) * score_scale
        highest = lax.optimization_barrier(jnp.max(scores, axis=-1, keepdims=True))
        weights = jnp.exp(scores - highest)
        totals = lax.optimization_barrier(jnp.sum(weights, axis=-1))
        rounded = lax.optimization_barrier(weights.astype(jnp.bfloat16)).astype(jnp.float32)
        mixture = jnp.einsum('hmqk,khe->hmqe', rounded, value_all) / totals[..., None]
        differ = mixture[:, 0] - lambdas[:, None, None] * mixture[:, 1]
        normed_heads = differ * lax.rsqrt(lax.optimization_barrier(jnp.mean(differ * differ, axis=-1, keepdims=True)) + 1e-05) * head_gain
        return jnp.transpose(normed_heads, (1, 0, 2)).reshape(query_rows, HEADS * value_width).astype(jnp.bfloat16)
    query_blocks = queries.reshape(SEQ // query_rows, query_rows, HEADS, 2, HD)
    heads_out = lax.map(attend, query_blocks).reshape(SEQ, HEADS * value_width)
    projected = jnp.dot(heads_out, w_out, preferred_element_type=jnp.float32)
    hidden_state = (residual.astype(jnp.float32) + projected).astype(jnp.bfloat16)
    stream_f = hidden_state.astype(jnp.float32)
    normed = (stream_f * lax.rsqrt(lax.optimization_barrier(jnp.mean(stream_f * stream_f, axis=-1, keepdims=True)) + 1e-05) * norm_gain).astype(jnp.bfloat16)
    group_width = FF // N_TP
    summed = jnp.zeros((SEQ, D), jnp.float32)
    for member in range(N_TP):
        lower = member * group_width
        gate_part = jnp.dot(normed, w_gate[:, lower:lower + group_width], preferred_element_type=jnp.float32)
        up_part = jnp.dot(normed, w_up[:, lower:lower + group_width], preferred_element_type=jnp.float32)
        hidden_part = (jax.nn.silu(gate_part) * up_part).astype(jnp.bfloat16)
        partial_sum = jnp.dot(hidden_part, w_down[lower:lower + group_width], preferred_element_type=jnp.float32)
        summed = summed + lax.optimization_barrier(partial_sum.astype(jnp.bfloat16)).astype(jnp.float32)
    return (stream_f + summed).astype(jnp.bfloat16)
```

```python
import functools

import jax
import jax.numpy as jnp
from jax import lax
from jax.experimental import pallas as pl
from jax.experimental.pallas import tpu as pltpu
from jax.sharding import Mesh
from jax.sharding import PartitionSpec as P

HD = 64
SP = ("sp_0", "sp_1")
SP_TP = ("sp_0", "sp_1", "tp")
LOWEST = -1e30
EXTRA = 16


def spread_queries(q, out_ref, at):
    rows = q.shape[0]
    lane = lax.broadcasted_iota(jnp.int32, q.shape, 1)
    zero = jnp.zeros_like(q)
    out_ref[pl.ds(at, rows), :] = jnp.where(lane < HD, q, zero)
    out_ref[pl.ds(at + rows, rows), :] = jnp.where(lane >= HD, q, zero)


def attend_tile(q2, keys, values_t, high_ref, acc_ref):
    scores = lax.dot_general(
        keys, q2, (((1,), (1,)), ((), ())), preferred_element_type=jnp.float32
    )
    before = high_ref[...]
    after = jnp.maximum(before, jnp.max(scores, axis=0, keepdims=True))
    shrink = jnp.exp(before - after)
    weights = jnp.exp(scores - after).astype(jnp.bfloat16)
    mixed = jnp.dot(values_t, weights, preferred_element_type=jnp.float32)
    acc_ref[...] = acc_ref[...] * shrink + mixed
    high_ref[...] = after


def attention_kernel(q_ref, k_ref, vt_ref, o_ref, lse_ref, q2, high, acc):
    groups, rows, _ = q_ref.shape
    width = vt_ref.shape[1] - EXTRA
    for g in range(groups):
        spread_queries(q_ref[g], q2, g * 2 * rows)
    high[...] = jnp.full_like(high, LOWEST)
    acc[...] = jnp.zeros_like(acc)

    def step(i, c):
        attend_tile(q2[...], k_ref[i], vt_ref[i], high, acc)
        return c

    lax.fori_loop(0, k_ref.shape[0], step, 0)
    for g in range(groups):
        cols = pl.ds(g * 2 * rows, 2 * rows)
        totals = acc[pl.ds(width, 1), cols]
        o_ref[g] = (acc[pl.ds(0, width), cols] / totals).astype(o_ref.dtype)
        lse_ref[g] = jnp.broadcast_to(high[:, cols] + jnp.log(totals), (8, 2 * rows))


def attention(q_all, k_all, vt_all):
    groups, rows, _ = q_all.shape
    width = vt_all.shape[1] - EXTRA
    columns = groups * 2 * rows
    return pl.pallas_call(
        attention_kernel,
        out_shape=(
            jax.ShapeDtypeStruct((groups, width, 2 * rows), jnp.bfloat16),
            jax.ShapeDtypeStruct((groups, 8, 2 * rows), jnp.float32),
        ),
        in_specs=[pl.BlockSpec(memory_space=pltpu.VMEM)] * 3,
        out_specs=[pl.BlockSpec(memory_space=pltpu.VMEM)] * 2,
        scratch_shapes=[
            pltpu.VMEM((columns, 2 * HD), jnp.bfloat16),
            pltpu.VMEM((1, columns), jnp.float32),
            pltpu.VMEM((width + EXTRA, columns), jnp.float32),
        ],
        cost_estimate=pl.CostEstimate(
            flops=30_000_000_000, bytes_accessed=8_000_000, transcendentals=16_000_000
        ),
        compiler_params=pltpu.CompilerParams(vmem_limit_bytes=56 * 2**20),
    )(q_all, k_all, vt_all)


def laid_out(parts, dim):
    parts = jnp.moveaxis(parts, 0, dim)
    dims = parts.shape
    return parts.reshape(*dims[:dim], dims[dim] * dims[dim + 1], *dims[dim + 2 :])


def gather_directly(shard, axis, dim):
    length = lax.axis_size(axis)
    parts = lax.all_to_all(
        jnp.broadcast_to(shard[None], (length, *shard.shape)), axis, 0, 0, tiled=True
    )
    return laid_out(parts, dim)


def summed_on_arrival(shard, axis):
    length = lax.axis_size(axis)
    parts = shard.reshape(length, shard.shape[0] // length, shard.shape[1])
    arrived = lax.all_to_all(parts, axis, split_axis=0, concat_axis=0, tiled=True)
    return arrived.astype(jnp.float32).sum(axis=0)


def per_device(
    residual, queries, key_pairs, values, lambdas, head_gain, w_out, norm_gain, w_gate, w_up, w_down
):
    local_rows = queries.shape[0]
    scaled_q = queries * jnp.bfloat16(HD**-0.5)
    k_all = lax.all_gather(key_pairs, "sp_0", axis=0)
    extra = jnp.concatenate(
        [jnp.ones((1, local_rows), jnp.bfloat16), jnp.zeros((EXTRA - 1, local_rows), jnp.bfloat16)]
    )
    vt = lax.all_gather(values.T, "sp_0", axis=0)
    vt_all = jnp.concatenate([vt, jnp.broadcast_to(extra, (vt.shape[0], *extra.shape))], axis=1)
    q_all = lax.all_gather(scaled_q, "sp_1", axis=0)
    mixed_part, lse_part = attention(q_all, k_all, vt_all)
    mixed_part = lax.all_to_all(mixed_part, "sp_1", 0, 0, tiled=True).astype(jnp.float32)
    lse_part = lax.all_to_all(lse_part, "sp_1", 0, 0, tiled=True)[:, :1]
    share = jnp.exp(lse_part - jnp.max(lse_part, axis=0, keepdims=True))
    share = share / jnp.sum(share, axis=0, keepdims=True)
    mixed = jnp.sum(mixed_part * share, axis=0)
    differ = mixed[:, :local_rows] - lambdas[0] * mixed[:, local_rows:]
    normed_heads = (
        differ
        * lax.rsqrt(jnp.mean(differ * differ, axis=0, keepdims=True) + 1e-05)
        * head_gain[:, None]
    )
    heads_out = normed_heads.T.astype(jnp.bfloat16)
    tp_index = lax.axis_index("tp")
    own_rows = local_rows // lax.axis_size("tp")
    own_begin = tp_index * own_rows
    token_heads = lax.all_to_all(heads_out, "tp", split_axis=0, concat_axis=1, tiled=True)
    projected = jnp.dot(token_heads, w_out, preferred_element_type=jnp.float32)
    residual_own = lax.dynamic_slice_in_dim(residual, own_begin, own_rows, 0)
    hidden_own = (residual_own.astype(jnp.float32) + projected).astype(jnp.bfloat16)
    stream_f = hidden_own.astype(jnp.float32)
    scaled = stream_f * lax.rsqrt(jnp.mean(stream_f * stream_f, axis=-1, keepdims=True) + 1e-05)
    normed_rows = gather_directly((scaled * norm_gain).astype(jnp.bfloat16), "tp", 0)
    unit_width = w_gate.shape[1]
    joined = jnp.concatenate([w_gate, w_up], axis=1)
    w_all = lax.all_gather(joined, SP, axis=0, tiled=True)
    both_sums = jnp.dot(normed_rows, w_all, preferred_element_type=jnp.float32)
    gate_sum = both_sums[:, :unit_width]
    up_sum = both_sums[:, unit_width:]
    hidden_units = (jax.nn.silu(gate_sum) * up_sum).astype(jnp.bfloat16)
    down_t = lax.all_gather(w_down.T, SP, axis=0, tiled=True)
    ffn_part = lax.dot_general(
        hidden_units, down_t, (((1,), (1,)), ((), ())), preferred_element_type=jnp.float32
    )
    ffn_out = summed_on_arrival(ffn_part.astype(jnp.bfloat16), "tp")
    return (hidden_own.astype(jnp.float32) + ffn_out).astype(jnp.bfloat16)


def solution(mesh):
    torus = Mesh(mesh.devices.reshape(8, 4, mesh.shape["tp"]), ("sp_0", "sp_1", "tp"))
    return jax.shard_map(
        per_device,
        mesh=torus,
        in_specs=(
            P(SP, None),
            P(SP, "tp"),
            P(SP, "tp"),
            P(SP, "tp"),
            P("tp"),
            P(),
            P(),
            P(),
            P(SP, "tp"),
            P(SP, "tp"),
            P("tp", SP),
        ),
        out_specs=P(SP_TP, None),
        check_vma=False,
    )
```

```python
import functools

import jax
import jax.numpy as jnp
from jax import lax
from jax.experimental import pallas as pl
from jax.experimental.pallas import tpu as pltpu
from jax.sharding import Mesh
from jax.sharding import PartitionSpec as P

HD = 64
SP = ("sp_0", "sp_1")
SP_TP = ("sp_0", "sp_1", "tp")
LOWEST = -1e30
EXTRA = 16
NZ = 8
NX = 4
MESH = pl.DeviceIdType.MESH


def spread_queries(q, out_ref, at):
    rows = q.shape[0]
    lane = lax.broadcasted_iota(jnp.int32, q.shape, 1)
    zero = jnp.zeros_like(q)
    out_ref[pl.ds(at, rows), :] = jnp.where(lane < HD, q, zero)
    out_ref[pl.ds(at + rows, rows), :] = jnp.where(lane >= HD, q, zero)


def attend_tile(q2, keys, values_t, high_ref, acc_ref):
    scores = lax.dot_general(
        keys, q2, (((1,), (1,)), ((), ())), preferred_element_type=jnp.float32
    )
    before = high_ref[...]
    after = jnp.maximum(before, jnp.max(scores, axis=0, keepdims=True))
    shrink = jnp.exp(before - after)
    weights = jnp.exp(scores - after).astype(jnp.bfloat16)
    mixed = jnp.dot(values_t, weights, preferred_element_type=jnp.float32)
    acc_ref[...] = acc_ref[...] * shrink + mixed
    high_ref[...] = after


class Ring:
    def __init__(self, axis, size, block, send, recv, steps):
        self.me = lax.axis_index(axis)
        self.axis, self.size, self.block = axis, size, block
        self.send, self.recv, self.steps = send, recv, steps

    def copy(self, way, step, at):
        target = lax.rem(self.me + (1 if way == 0 else self.size - 1), self.size)
        src, dst = self.block(way, step, at)
        return pltpu.make_async_remote_copy(
            src_ref=src,
            dst_ref=dst,
            send_sem=self.send.at[way, step],
            recv_sem=self.recv.at[way, step],
            device_id={self.axis: target},
            device_id_type=MESH,
        )

    def start(self, step):
        for way in (0, 1):
            if step < self.steps[way]:
                self.copy(way, step, 0).start()

    def arrived(self, step):
        for way in (0, 1):
            if step < self.steps[way]:
                self.copy(way, step, 1).wait_recv()

    def sent(self):
        for way in (0, 1):
            for step in range(self.steps[way]):
                self.copy(way, step, 0).wait_send()


def attention_kernel(
    q_ref, k_ref, vt_ref, w_ref, lam_ref, gain_ref,
    heads_ref, wall_ref,
    qb, kb, vb, q2, high, acc, osend, lsend, orecv, lrecv,
    q_sems, k_sems, v_sems, a_sems, az_sems, bz_sems, bx_sems, o_sems, l_sems, local_sems,
):
    z, x = lax.axis_index("sp_0"), lax.axis_index("sp_1")
    rows = q_ref.shape[0]
    width = vt_ref.shape[0]
    half = w_ref.shape[0] // 2
    quarter = half // 2
    columns = 2 * rows

    def slot(way, step):
        return 0 if step == 0 else 2 * step - 1 if way == 0 else 7 if step == 4 else 2 * step

    def k_block(way, step, at):
        return (k_ref if step + at == 0 else kb.at[slot(way, step + at)], kb.at[slot(way, step + 1)])

    def v_block(way, step, at):
        inside = vb.at[slot(way, step + at), pl.ds(0, width), :]
        return (vt_ref if step + at == 0 else inside, vb.at[slot(way, step + 1), pl.ds(0, width), :])

    def origin(way, step):
        return lax.rem(z + (NZ - step if way == 0 else step), NZ)

    def az_block(way, step, at):
        xs = pl.ds(0, NX) if step < 3 else pl.ds(0 if way == 0 else NX // 2, NX // 2)
        ref = wall_ref.at[origin(way, step + at), xs, pl.ds(0, half), :]
        return (ref, ref)

    def bz_block(way, step, at):
        rs = pl.ds(half, half) if step < 3 else pl.ds(half if way == 0 else half + quarter, quarter)
        ref = wall_ref.at[origin(way, step + at), x, rs, :]
        return (w_ref.at[pl.ds(half, half)] if step + at == 0 else ref, ref)

    def bx_block(way, step, at):
        from_x = lax.rem(x + (NX - step - at if way == 0 else step + at), NX)
        zs = pl.ds(0, NZ) if step == 0 else pl.ds(0 if way == 0 else NZ // 2, NZ // 2)
        ref = wall_ref.at[zs, from_x, pl.ds(half, half), :]
        return (ref, ref)

    kring = Ring("sp_0", NZ, k_block, k_sems.at[0], k_sems.at[1], (4, 3))
    vring = Ring("sp_0", NZ, v_block, v_sems.at[0], v_sems.at[1], (3, 4))
    azring = Ring("sp_0", NZ, az_block, az_sems.at[0], az_sems.at[1], (4, 4))
    bzring = Ring("sp_0", NZ, bz_block, bz_sems.at[0], bz_sems.at[1], (4, 4))
    bxring = Ring("sp_1", NX, bx_block, bx_sems.at[0], bx_sems.at[1], (2, 2))

    def to_peer(g, src, dst, sems):
        return pltpu.make_async_remote_copy(
            src_ref=src,
            dst_ref=dst,
            send_sem=sems.at[0, g - 1],
            recv_sem=sems.at[1, g - 1],
            device_id={"sp_1": lax.rem(x + g, NX)},
            device_id_type=MESH,
        )

    def q_copy(g):
        return to_peer(g, q_ref, qb.at[NX - 1 - g], q_sems)

    def a_copy(g, from_x):
        return to_peer(g, w_ref.at[pl.ds(0, half)], wall_ref.at[z, from_x, pl.ds(0, half), :], a_sems)

    def o_copy(g):
        return to_peer(g, osend.at[g - 1], orecv.at[g - 1], o_sems)

    def l_copy(g):
        return to_peer(g, lsend.at[g - 1], lrecv.at[g - 1], l_sems)

    barrier = pltpu.get_barrier_semaphore()
    for step in (1, NZ - 1):
        pl.semaphore_signal(
            barrier, inc=1, device_id={"sp_0": lax.rem(z + step, NZ)}, device_id_type=MESH
        )
    for step in range(1, NX):
        pl.semaphore_signal(
            barrier, inc=1, device_id={"sp_1": lax.rem(x + step, NX)}, device_id_type=MESH
        )
    pl.semaphore_wait(barrier, 2 + NX - 1)

    for g in (2, 1, 3):
        q_copy(g).start()
    kring.start(0)
    vring.start(0)
    bzring.start(0)
    for g in (2, 1, 3):
        a_copy(g, x).start()
    own_w = pltpu.make_async_copy(w_ref, wall_ref.at[z, x], local_sems.at[0])
    own_k = pltpu.make_async_copy(k_ref, kb.at[0], local_sems.at[1])
    own_v = pltpu.make_async_copy(vt_ref, vb.at[0, pl.ds(0, width), :], local_sems.at[2])
    own_w.start()
    own_k.start()
    own_v.start()
    one_row = lax.broadcasted_iota(jnp.int32, (EXTRA, rows), 0) == 0
    for i in range(NZ):
        vb[i, pl.ds(width, EXTRA), :] = jnp.where(one_row, 1.0, 0.0).astype(vb.dtype)
    spread_queries(q_ref[...], q2, 0)
    high[...] = jnp.full_like(high, LOWEST)
    acc[...] = jnp.zeros_like(acc)
    own_w.wait()
    own_k.wait()
    own_v.wait()
    for g in (1, 3, 2):
        q_copy(g).wait_recv()
    for g in range(1, NX):
        spread_queries(qb[g - 1], q2, g * columns)

    def a_arrived():
        for g in range(1, NX):
            a_copy(g, lax.rem(x + NX - g, NX)).wait_recv()

    events = {
        1: [lambda: kv_step(0), lambda: b_step(0)],
        2: [a_arrived, lambda: azring.start(0), lambda: b_step(1)],
        3: [lambda: kv_step(1), lambda: b_step(2)],
        4: [lambda: b_step(3), lambda: a_step(0)],
        5: [lambda: kv_step(2)],
        6: [lambda: a_step(1)],
        7: [lambda: kv_step(3)],
    }

    def kv_step(s):
        kring.arrived(s)
        vring.arrived(s)
        if s < 3:
            kring.start(s + 1)
            vring.start(s + 1)

    def b_step(s):
        bzring.arrived(s)
        if s < 3:
            bzring.start(s + 1)
        else:
            bxring.start(0)

    def a_step(s):
        azring.arrived(s)
        if s < 3:
            azring.start(s + 1)

    def tile(i, carry):
        for at, todo in events.items():

            @pl.when(i == at)
            def _():
                for act in todo:
                    act()

        attend_tile(q2[...], kb[i], vb[i], high, acc)
        return carry

    lax.fori_loop(0, NZ, tile, 0)

    def result(g):
        cols = pl.ds(g * columns, columns)
        totals = acc[pl.ds(width, 1), cols]
        return acc[pl.ds(0, width), cols] / totals, high[:, cols] + jnp.log(totals)

    before = None
    for g in (2, 1, 3):
        mix, lse = result(g)
        osend[g - 1] = mix.astype(osend.dtype)
        lsend[g - 1] = jnp.broadcast_to(lse, lsend.shape[1:])
        if before is not None:
            o_copy(before).start()
            l_copy(before).start()
        before = g
    mix, lse = result(0)
    o_copy(before).start()
    l_copy(before).start()
    a_step(2)
    bxring.arrived(0)
    bxring.start(1)
    for g in range(1, NX):
        o_copy(g).wait_recv()
        l_copy(g).wait_recv()
    lses = [lse] + [lrecv[g][:1] for g in range(NX - 1)]
    top = functools.reduce(jnp.maximum, lses)
    shares = [jnp.exp(one - top) for one in lses]
    mix = mix * shares[0]
    for g in range(NX - 1):
        mix = mix + orecv[g].astype(jnp.float32) * shares[g + 1]
    mix = mix / functools.reduce(jnp.add, shares)
    differ = mix[:, :rows] - lam_ref[0] * mix[:, rows:]
    square = jnp.mean(differ * differ, axis=0, keepdims=True)
    heads = differ * lax.rsqrt(square + 1e-05) * gain_ref[...]
    heads_ref[...] = heads.T.astype(heads_ref.dtype)

    azring.arrived(3)
    bxring.arrived(1)
    for ring in (kring, vring, azring, bzring, bxring):
        ring.sent()
    for g in range(1, NX):
        for copy in (q_copy(g), a_copy(g, x), o_copy(g), l_copy(g)):
            copy.wait_send()


def attention(q, k, vt, w, lambdas, gain):
    rows = q.shape[0]
    width = vt.shape[0]
    columns = NX * 2 * rows
    vmem = pl.BlockSpec(memory_space=pltpu.VMEM)
    dma = pltpu.SemaphoreType.DMA
    return pl.pallas_call(
        attention_kernel,
        out_shape=(
            jax.ShapeDtypeStruct((rows, width), jnp.bfloat16),
            jax.ShapeDtypeStruct((NZ, NX, *w.shape), jnp.bfloat16),
        ),
        in_specs=[vmem] * 4 + [pl.BlockSpec(memory_space=pltpu.SMEM), vmem],
        out_specs=[vmem] * 2,
        scratch_shapes=[
            pltpu.VMEM((NX - 1, rows, 2 * HD), jnp.bfloat16),
            pltpu.VMEM((NZ, rows, 2 * HD), jnp.bfloat16),
            pltpu.VMEM((NZ, width + EXTRA, rows), jnp.bfloat16),
            pltpu.VMEM((columns, 2 * HD), jnp.bfloat16),
            pltpu.VMEM((1, columns), jnp.float32),
            pltpu.VMEM((width + EXTRA, columns), jnp.float32),
            pltpu.VMEM((NX - 1, width, 2 * rows), jnp.bfloat16),
            pltpu.VMEM((NX - 1, 8, 2 * rows), jnp.float32),
            pltpu.VMEM((NX - 1, width, 2 * rows), jnp.bfloat16),
            pltpu.VMEM((NX - 1, 8, 2 * rows), jnp.float32),
            dma((2, NX - 1)),
            dma((2, 2, 4)),
            dma((2, 2, 4)),
            dma((2, NX - 1)),
            dma((2, 2, 4)),
            dma((2, 2, 4)),
            dma((2, 2, 2)),
            dma((2, NX - 1)),
            dma((2, NX - 1)),
            dma((3,)),
        ],
        cost_estimate=pl.CostEstimate(
            flops=30_000_000_000, bytes_accessed=8_000_000, transcendentals=16_000_000
        ),
        compiler_params=pltpu.CompilerParams(
            vmem_limit_bytes=60 * 2**20, collective_id=0, has_side_effects=True
        ),
    )(q, k, vt, w, lambdas, gain)


def laid_out(parts, dim):
    parts = jnp.moveaxis(parts, 0, dim)
    dims = parts.shape
    return parts.reshape(*dims[:dim], dims[dim] * dims[dim + 1], *dims[dim + 2 :])


def gather_directly(shard, axis, dim):
    length = lax.axis_size(axis)
    parts = lax.all_to_all(
        jnp.broadcast_to(shard[None], (length, *shard.shape)), axis, 0, 0, tiled=True
    )
    return laid_out(parts, dim)


def summed_on_arrival(shard, axis):
    length = lax.axis_size(axis)
    parts = shard.reshape(length, shard.shape[0] // length, shard.shape[1])
    arrived = lax.all_to_all(parts, axis, split_axis=0, concat_axis=0, tiled=True)
    return arrived.astype(jnp.float32).sum(axis=0)


def per_device(
    residual, queries, key_pairs, values, lambdas, head_gain, w_out, norm_gain, w_gate, w_up, w_down
):
    local_rows = queries.shape[0]
    scaled_q = queries * jnp.bfloat16(HD**-0.5)
    joined = jnp.concatenate([w_gate, w_up], axis=1)
    down_t = lax.all_gather(w_down.T, SP, axis=0, tiled=True)
    heads_out, w_all = attention(
        scaled_q, key_pairs, values.T, joined, lambdas, head_gain[:, None]
    )
    w_all = w_all.reshape(-1, w_all.shape[-1])
    tp_index = lax.axis_index("tp")
    own_rows = local_rows // lax.axis_size("tp")
    own_begin = tp_index * own_rows
    token_heads = lax.all_to_all(heads_out, "tp", split_axis=0, concat_axis=1, tiled=True)
    projected = jnp.dot(token_heads, w_out, preferred_element_type=jnp.float32)
    residual_own = lax.dynamic_slice_in_dim(residual, own_begin, own_rows, 0)
    hidden_own = (residual_own.astype(jnp.float32) + projected).astype(jnp.bfloat16)
    stream_f = hidden_own.astype(jnp.float32)
    scaled = stream_f * lax.rsqrt(jnp.mean(stream_f * stream_f, axis=-1, keepdims=True) + 1e-05)
    normed_rows = gather_directly((scaled * norm_gain).astype(jnp.bfloat16), "tp", 0)
    unit_width = w_gate.shape[1]
    both_sums = jnp.dot(normed_rows, w_all, preferred_element_type=jnp.float32)
    gate_sum = both_sums[:, :unit_width]
    up_sum = both_sums[:, unit_width:]
    hidden_units = (jax.nn.silu(gate_sum) * up_sum).astype(jnp.bfloat16)
    ffn_part = lax.dot_general(
        hidden_units, down_t, (((1,), (1,)), ((), ())), preferred_element_type=jnp.float32
    )
    ffn_out = summed_on_arrival(ffn_part.astype(jnp.bfloat16), "tp")
    return (hidden_own.astype(jnp.float32) + ffn_out).astype(jnp.bfloat16)


def solution(mesh):
    torus = Mesh(mesh.devices.reshape(8, 4, mesh.shape["tp"]), ("sp_0", "sp_1", "tp"))
    return jax.shard_map(
        per_device,
        mesh=torus,
        in_specs=(
            P(SP, None),
            P(SP, "tp"),
            P(SP, "tp"),
            P(SP, "tp"),
            P("tp"),
            P(),
            P(),
            P(),
            P(SP, "tp"),
            P(SP, "tp"),
            P("tp", SP),
        ),
        out_specs=P(SP_TP, None),
        check_vma=False,
    )
```

```python
import functools

import jax
import jax.numpy as jnp
from jax import lax
from jax.experimental import pallas as pl
from jax.experimental.pallas import tpu as pltpu
from jax.sharding import Mesh
from jax.sharding import PartitionSpec as P

HD = 64
SP = ("sp_0", "sp_1")
SP_TP = ("sp_0", "sp_1", "tp")
LOWEST = -1e30
EXTRA = 16
NZ = 8
NX = 4
NY = 4
NT = 8
MESH = pl.DeviceIdType.MESH


def spread_queries(q, out_ref, at):
    rows = q.shape[0]
    lane = lax.broadcasted_iota(jnp.int32, q.shape, 1)
    zero = jnp.zeros_like(q)
    out_ref[pl.ds(at, rows), :] = jnp.where(lane < HD, q, zero)
    out_ref[pl.ds(at + rows, rows), :] = jnp.where(lane >= HD, q, zero)


def attend_tile(q2, keys, values_t, high_ref, acc_ref):
    scores = lax.dot_general(
        keys, q2, (((1,), (1,)), ((), ())), preferred_element_type=jnp.float32
    )
    before = high_ref[...]
    after = jnp.maximum(before, jnp.max(scores, axis=0, keepdims=True))
    shrink = jnp.exp(before - after)
    weights = jnp.exp(scores - after).astype(jnp.bfloat16)
    mixed = jnp.dot(values_t, weights, preferred_element_type=jnp.float32)
    acc_ref[...] = acc_ref[...] * shrink + mixed
    high_ref[...] = after


class Ring:
    def __init__(self, target, block, send, recv, steps):
        self.target, self.block = target, block
        self.send, self.recv, self.steps = send, recv, steps

    def copy(self, way, step, at):
        src, dst = self.block(way, step, at)
        return pltpu.make_async_remote_copy(
            src_ref=src,
            dst_ref=dst,
            send_sem=self.send.at[way, step],
            recv_sem=self.recv.at[way, step],
            device_id=self.target(way),
            device_id_type=MESH,
        )

    def start(self, step):
        for way in (0, 1):
            if step < self.steps[way]:
                self.copy(way, step, 0).start()

    def arrived(self, step):
        for way in (0, 1):
            if step < self.steps[way]:
                self.copy(way, step, 1).wait_recv()

    def sent(self):
        for way in (0, 1):
            for step in range(self.steps[way]):
                self.copy(way, step, 0).wait_send()


class Gather:
    def __init__(self, shard, whole, z, x, z_target, x_target, z_sems, one_sems, two_sems):
        self.shard, self.whole, self.z, self.x = shard, whole, z, x
        self.x_target, self.one, self.two = x_target, one_sems, two_sems
        self.rows = shard.shape[0]
        self.ring = Ring(z_target, self.z_block, z_sems.at[0], z_sems.at[1], (4, 4))

    def origin(self, index):
        step = (index + 1) // 2
        return lax.rem(self.z + (NZ - step if index % 2 else step), NZ)

    def z_block(self, way, step, at):
        half = self.rows // 2
        rows = pl.ds(0, self.rows) if step < 3 else pl.ds(half * way, half)
        origin = lax.rem(self.z + (NZ - step - at if way == 0 else step + at), NZ)
        ref = self.whole(origin, self.x, rows)
        return (self.shard if step + at == 0 else ref, ref)

    def along_x(self, src, dst, sems, way, index):
        return pltpu.make_async_remote_copy(
            src_ref=src,
            dst_ref=dst,
            send_sem=sems.at[0, way, index],
            recv_sem=sems.at[1, way, index],
            device_id=self.x_target(way),
            device_id_type=MESH,
        )

    def hop(self, number, way, index, at):
        step = number - 1 + at
        from_x = lax.rem(self.x + (NX - step if way == 0 else step), NX)
        ref = self.whole(self.origin(index), from_x, pl.ds(0, self.rows))
        own = number == 1 and at == 0 and index == 0
        sems = self.one if number == 1 else self.two
        return self.along_x(self.shard if own else ref, ref, sems, way, index)

    def members(self, k):
        return [0] if k == 0 else [7] if k == 4 else [2 * k - 1, 2 * k]

    def second_way(self, index):
        return 0 if index in (0, 1, 3, 5) else 1

    def step(self, k):
        if k > 0:
            self.ring.arrived(k - 1)
        if k < 4:
            self.ring.start(k)
        for index in self.members(k):
            for way in (0, 1):
                self.hop(1, way, index, 0).start()

    def forward(self, k):
        for index in self.members(k):
            for way in (0, 1):
                self.hop(1, way, index, 1).wait_recv()
            self.hop(2, self.second_way(index), index, 0).start()

    def done(self):
        for index in range(NZ):
            self.hop(2, self.second_way(index), index, 1).wait_recv()

    def sent(self):
        self.ring.sent()
        for index in range(NZ):
            for way in (0, 1):
                self.hop(1, way, index, 0).wait_send()
            self.hop(2, self.second_way(index), index, 0).wait_send()


def layer_kernel(
    q_ref, k_ref, vt_ref, w_ref, wd_ref, lam_ref, gain_ref, norm_gain_ref, res_ref, wout_ref,
    out_ref,
    qb, kb, vb, q2, high, acc, osend, lsend, orecv, lrecv, orelay,
    wall, down, wout, res, heads, th, normed, hidden, units, parts, pb, pr, fs, fr, relay,
    q_sems, k_sems, v_sems, ax_sems, az_sems, bz_sems, b1_sems, b2_sems,
    cz_sems, c1_sems, c2_sems, o_sems, l_sems, or_sems, local_sems,
    h_sems, y_sems, p_sems, c_sems, r_sems, rr_sems,
):
    z, x, t = lax.axis_index("sp_0"), lax.axis_index("sp_1"), lax.axis_index("tp")
    y, core = t // 2, lax.rem(t, 2)
    rows = q_ref.shape[0]
    width = vt_ref.shape[0]
    half = w_ref.shape[0] // 2
    columns = 2 * rows
    own = rows // NT
    unit_width = wd_ref.shape[1]

    def z_target(way):
        return {"sp_0": lax.rem(z + (1 if way == 0 else NZ - 1), NZ)}

    def x_target(way):
        return {"sp_1": lax.rem(x + (1 if way == 0 else NX - 1), NX)}

    def chip(offset):
        return lax.rem(y + offset, NY)

    def y_target(way):
        return {"tp": chip(1 if way == 0 else NY - 1) * 2 + core}

    partner = {"tp": t + 1 - 2 * core}

    def slot(way, step):
        return 0 if step == 0 else 2 * step - 1 if way == 0 else 7 if step == 4 else 2 * step

    def k_block(way, step, at):
        src = k_ref if step + at == 0 else kb.at[slot(way, step + at)]
        return (src, kb.at[slot(way, step + 1)])

    def v_block(way, step, at):
        inside = vb.at[slot(way, step + at), pl.ds(0, width), :]
        src = vt_ref if step + at == 0 else inside
        return (src, vb.at[slot(way, step + 1), pl.ds(0, width), :])

    def q_block(way, step, at):
        part = pl.ds(0, rows) if step == 0 else pl.ds(way * (rows // 2), rows // 2)
        place = lambda hops: (2 if way == 0 else 0) if hops == 1 else 1
        src = q_ref if step + at == 0 else qb.at[place(step + at), part, :]
        return (src, qb.at[place(step + 1), part, :])

    def ax_block(way, step, at):
        part = pl.ds(0, half) if step == 0 else pl.ds(way * (half // 2), half // 2)
        from_x = lax.rem(x + (NX - step - at if way == 0 else step + at), NX)
        ref = wall.at[z, from_x, part, :]
        return (w_ref.at[pl.ds(0, half)] if step + at == 0 else ref, ref)

    def az_block(way, step, at):
        xs = pl.ds(0, NX) if step < 3 else pl.ds(0 if way == 0 else NX // 2, NX // 2)
        origin = lax.rem(z + (NZ - step - at if way == 0 else step + at), NZ)
        ref = wall.at[origin, xs, pl.ds(0, half), :]
        return (ref, ref)

    def b_whole(from_z, from_x, part):
        return wall.at[from_z, from_x, pl.ds(half + part.start, part.size), :]

    def c_whole(from_z, from_x, part):
        return down.at[from_z, from_x, part, :]

    def o_block(way, step, at):
        part = pl.ds(way * (width // 2), width // 2)
        if step == 0:
            return (osend.at[1, part, :], orelay.at[way])
        return (orelay.at[way], orecv.at[1, part, :])

    kring = Ring(z_target, k_block, k_sems.at[0], k_sems.at[1], (4, 3))
    vring = Ring(z_target, v_block, v_sems.at[0], v_sems.at[1], (3, 4))
    qring = Ring(x_target, q_block, q_sems.at[0], q_sems.at[1], (2, 2))
    axring = Ring(x_target, ax_block, ax_sems.at[0], ax_sems.at[1], (2, 2))
    azring = Ring(z_target, az_block, az_sems.at[0], az_sems.at[1], (4, 4))
    oring = Ring(x_target, o_block, or_sems.at[0], or_sems.at[1], (2, 2))
    later = Gather(
        w_ref.at[pl.ds(half, half)], b_whole, z, x, z_target, x_target, bz_sems, b1_sems, b2_sems
    )
    lowest = Gather(wd_ref, c_whole, z, x, z_target, x_target, cz_sems, c1_sems, c2_sems)

    def x_peer(g, src, dst, sems):
        return pltpu.make_async_remote_copy(
            src_ref=src,
            dst_ref=dst,
            send_sem=sems.at[0, g - 1],
            recv_sem=sems.at[1, g - 1],
            device_id={"sp_1": lax.rem(x + g, NX)},
            device_id_type=MESH,
        )

    def o_copy(g):
        return x_peer(g, osend.at[g - 1], orecv.at[g - 1], o_sems)

    def l_copy(g):
        return x_peer(g, lsend.at[g - 1], lrecv.at[g - 1], l_sems)

    barrier = pltpu.get_barrier_semaphore()
    greeted = [{"sp_0": lax.rem(z + s, NZ)} for s in (1, NZ - 1)]
    greeted += [{"sp_1": lax.rem(x + s, NX)} for s in range(1, NX)]
    greeted += [{"tp": lax.rem(t + s, NT)} for s in range(1, NT)]
    for device in greeted:
        pl.semaphore_signal(barrier, inc=1, device_id=device, device_id_type=MESH)
    pl.semaphore_wait(barrier, len(greeted))

    qring.start(0)
    kring.start(0)
    vring.start(0)
    axring.start(0)
    later.step(0)
    locals_ = [
        pltpu.make_async_copy(src, dst, local_sems.at[i])
        for i, (src, dst) in enumerate(
            (
                (k_ref, kb.at[0]),
                (vt_ref, vb.at[0, pl.ds(0, width), :]),
                (w_ref, wall.at[z, x]),
                (wd_ref, down.at[z, x]),
                (res_ref.at[pl.ds(pl.multiple_of(t * own, own), own), :], res),
                (wout_ref, wout),
            )
        )
    ]
    for copy in locals_:
        copy.start()
    one_row = lax.broadcasted_iota(jnp.int32, (EXTRA, rows), 0) == 0
    for i in range(NZ):
        vb[i, pl.ds(width, EXTRA), :] = jnp.where(one_row, 1.0, 0.0).astype(vb.dtype)
    spread_queries(q_ref[...], q2, 0)
    high[...] = jnp.full_like(high, LOWEST)
    acc[...] = jnp.zeros_like(acc)
    for copy in locals_[:4]:
        copy.wait()

    def group_tile(g):
        cols = pl.ds(g * columns, columns)
        attend_tile(q2[cols, :], kb[0], vb[0], high.at[:, cols], acc.at[:, cols])

    def kv_step(s):
        kring.arrived(s)
        vring.arrived(s)
        if s < 3:
            kring.start(s + 1)
            vring.start(s + 1)

    def a_step(s):
        azring.arrived(s)
        if s < 3:
            azring.start(s + 1)

    group_tile(0)
    qring.arrived(0)
    qring.start(1)
    axring.arrived(0)
    axring.start(1)
    for g in (1, 3):
        spread_queries(qb[g - 1], q2, g * columns)
        group_tile(g)
    kv_step(0)
    later.step(1)
    later.forward(0)
    qring.arrived(1)
    spread_queries(qb[1], q2, 2 * columns)
    group_tile(2)
    axring.arrived(1)
    azring.start(0)

    events = {
        2: [lambda: later.step(2), lambda: later.forward(1)],
        3: [lambda: kv_step(1)],
        4: [lambda: a_step(0), lambda: later.step(3), lambda: later.forward(2)],
        5: [lambda: kv_step(2)],
        6: [lambda: later.step(4), lambda: later.forward(3), lambda: a_step(1), lambda: lowest.step(0)],
        7: [lambda: kv_step(3)],
    }

    def tile(i, carry):
        for at, todo in events.items():

            @pl.when(i == at)
            def _():
                for act in todo:
                    act()

        attend_tile(q2[...], kb[i], vb[i], high, acc)
        return carry

    lax.fori_loop(1, NZ, tile, 0)

    def result(g):
        cols = pl.ds(g * columns, columns)
        totals = acc[pl.ds(width, 1), cols]
        return acc[pl.ds(0, width), cols] / totals, high[:, cols] + jnp.log(totals)

    def stored(g):
        mix, lse = result(g)
        osend[g - 1] = mix.astype(osend.dtype)
        lsend[g - 1] = jnp.broadcast_to(lse, lsend.shape[1:])

    stored(2)
    lowest.step(1)
    lowest.forward(0)
    stored(1)
    oring.start(0)
    l_copy(2).start()
    stored(3)
    o_copy(1).start()
    l_copy(1).start()
    mix, lse = result(0)
    o_copy(3).start()
    l_copy(3).start()
    later.forward(4)
    a_step(2)
    oring.arrived(0)
    oring.start(1)
    lowest.step(2)
    lowest.forward(1)
    for g in (1, 3):
        o_copy(g).wait_recv()
    for g in range(1, NX):
        l_copy(g).wait_recv()
    oring.arrived(1)
    lses = [lse] + [lrecv[g][:1] for g in range(NX - 1)]
    top = functools.reduce(jnp.maximum, lses)
    shares = [jnp.exp(one - top) for one in lses]
    mix = mix * shares[0]
    for g in range(NX - 1):
        mix = mix + orecv[g].astype(jnp.float32) * shares[g + 1]
    mix = mix / functools.reduce(jnp.add, shares)
    differ = mix[:, :rows] - lam_ref[0] * mix[:, rows:]
    square = jnp.mean(differ * differ, axis=0, keepdims=True)
    mine = differ * lax.rsqrt(square + 1e-05) * gain_ref[...]
    heads[...] = mine.T.astype(heads.dtype)
    lowest.step(3)
    lowest.forward(2)

    def own_rows(index):
        return pl.ds(pl.multiple_of(index * own, own), own)

    def h_copy(d, to, home):
        return pltpu.make_async_remote_copy(
            src_ref=heads.at[own_rows(to), :],
            dst_ref=th.at[home],
            send_sem=h_sems.at[0, d - 1],
            recv_sem=h_sems.at[1, d - 1],
            device_id={"tp": to},
            device_id_type=MESH,
        )

    for d in range(1, NT):
        h_copy(d, lax.rem(t + d, NT), t).start()
    th[t] = heads[own_rows(t), :]
    lowest.step(4)
    lowest.forward(3)
    for copy in locals_[4:]:
        copy.wait()
    for d in range(1, NT):
        h_copy(d, lax.rem(t + d, NT), lax.rem(t + NT - d, NT)).wait_recv()
    token_heads = jnp.concatenate([th[h] for h in range(NT)], axis=1)
    projected = jnp.dot(token_heads, wout[...], preferred_element_type=jnp.float32)
    stream = (res[...].astype(jnp.float32) + projected).astype(jnp.bfloat16)
    hidden[...] = stream
    stream = stream.astype(jnp.float32)
    scale = lax.rsqrt(jnp.mean(stream * stream, axis=-1, keepdims=True) + 1e-05)
    normed[t] = (stream * scale * norm_gain_ref[...]).astype(normed.dtype)

    def y_block(way, step, at):
        part = pl.ds(0, own) if step == 0 else pl.ds(way * (own // 2), own // 2)
        ref = normed.at[chip(NY - step - at if way == 0 else step + at) * 2 + core, part, :]
        return (ref, ref)

    yring = Ring(y_target, y_block, y_sems.at[0], y_sems.at[1], (2, 2))
    shared = ((0, 0, own), (NY - 1, 0, own), (1, 0, own), (2, 0, own // 2), (2, own // 2, own // 2))

    def p_copy(number, of_core):
        offset, first, count = shared[number]
        ref = normed.at[chip(offset) * 2 + of_core, pl.ds(first, count), :]
        return pltpu.make_async_remote_copy(
            src_ref=ref,
            dst_ref=ref,
            send_sem=p_sems.at[0, number],
            recv_sem=p_sems.at[1, number],
            device_id=partner,
            device_id_type=MESH,
        )

    yring.start(0)
    p_copy(0, core).start()
    lowest.forward(4)
    yring.arrived(0)
    yring.start(1)
    p_copy(1, core).start()
    p_copy(2, core).start()
    yring.arrived(1)
    p_copy(3, core).start()
    p_copy(4, core).start()
    later.done()
    azring.arrived(3)
    for number in range(len(shared)):
        p_copy(number, 1 - core).wait_recv()
    sums = jnp.dot(
        normed[...].reshape(rows, -1),
        wall[...].reshape(-1, wall.shape[-1]),
        preferred_element_type=jnp.float32,
    )
    gate, up = sums[:, :unit_width], sums[:, unit_width:]
    gated = gate / (1.0 + jnp.exp(-gate)) * up
    units[...] = gated.astype(units.dtype).reshape(units.shape)
    lowest.done()

    def piece(offset):
        lhs = units[pl.ds(chip(offset) * 2, 2)].reshape(2 * own, unit_width)
        part = lax.dot_general(
            lhs,
            down[...].reshape(-1, unit_width),
            (((1,), (1,)), ((), ())),
            preferred_element_type=jnp.float32,
        )
        parts[offset] = part.reshape(parts.shape[1:])
        pb[offset] = parts[offset, 1 - core].astype(pb.dtype)

    def pair_copy(offset):
        return pltpu.make_async_remote_copy(
            src_ref=pb.at[offset],
            dst_ref=pr.at[offset],
            send_sem=c_sems.at[0, offset],
            recv_sem=c_sems.at[1, offset],
            device_id=partner,
            device_id_type=MESH,
        )

    def paired(offset):
        pair_copy(offset).wait_recv()
        return parts[offset, core] + pr[offset].astype(jnp.float32)

    def r_block(way, step, at):
        return (fs.at[1 if way == 0 else NY - 1], fr.at[way])

    def rr_block(way, step, at):
        part = pl.ds(way * (own // 2), own // 2)
        if step == 0:
            return (fs.at[2, part, :], relay.at[way])
        return (relay.at[way], fr.at[2, part, :])

    rring = Ring(y_target, r_block, r_sems.at[0], r_sems.at[1], (1, 1))
    rrring = Ring(y_target, rr_block, rr_sems.at[0], rr_sems.at[1], (2, 2))
    piece(2)
    piece(3)
    pair_copy(2).start()
    piece(1)
    pair_copy(3).start()
    fs[2] = paired(2).astype(fs.dtype)
    piece(0)
    pair_copy(1).start()
    rrring.start(0)
    fs[3] = paired(3).astype(fs.dtype)
    fs[1] = paired(1).astype(fs.dtype)
    pair_copy(0).start()
    rring.start(0)
    total = hidden[...].astype(jnp.float32) + paired(0)
    rrring.arrived(0)
    rrring.start(1)
    rring.arrived(0)
    total = total + fr[0].astype(jnp.float32) + fr[1].astype(jnp.float32)
    rrring.arrived(1)
    out_ref[...] = (total + fr[2].astype(jnp.float32)).astype(out_ref.dtype)

    for ring in (kring, vring, qring, axring, azring, oring, later, lowest, yring, rring, rrring):
        ring.sent()
    for g in (1, 3):
        o_copy(g).wait_send()
    for g in range(1, NX):
        l_copy(g).wait_send()
    for d in range(1, NT):
        h_copy(d, lax.rem(t + d, NT), t).wait_send()
    for number in range(len(shared)):
        p_copy(number, core).wait_send()
    for offset in range(NY):
        pair_copy(offset).wait_send()


def layer(q, k, vt, w, wd, lambdas, gain, norm_gain, residual, w_out):
    rows = q.shape[0]
    width = vt.shape[0]
    model = residual.shape[1]
    columns = NX * 2 * rows
    own = rows // NT
    units = wd.shape[1]
    vmem = pl.BlockSpec(memory_space=pltpu.VMEM)
    smem = pl.BlockSpec(memory_space=pltpu.SMEM)
    hbm = pl.BlockSpec(memory_space=pl.ANY)
    dma = pltpu.SemaphoreType.DMA
    short, long = jnp.bfloat16, jnp.float32
    return pl.pallas_call(
        layer_kernel,
        out_shape=jax.ShapeDtypeStruct((own, model), short),
        in_specs=[vmem] * 5 + [smem, vmem, vmem, hbm, hbm],
        out_specs=vmem,
        scratch_shapes=[
            pltpu.VMEM((NX - 1, rows, 2 * HD), short),
            pltpu.VMEM((NZ, rows, 2 * HD), short),
            pltpu.VMEM((NZ, width + EXTRA, rows), short),
            pltpu.VMEM((columns, 2 * HD), short),
            pltpu.VMEM((1, columns), long),
            pltpu.VMEM((width + EXTRA, columns), long),
            pltpu.VMEM((NX - 1, width, 2 * rows), short),
            pltpu.VMEM((NX - 1, 8, 2 * rows), long),
            pltpu.VMEM((NX - 1, width, 2 * rows), short),
            pltpu.VMEM((NX - 1, 8, 2 * rows), long),
            pltpu.VMEM((2, width // 2, 2 * rows), short),
            pltpu.VMEM((NZ, NX, *w.shape), short),
            pltpu.VMEM((NZ, NX, *wd.shape), short),
            pltpu.VMEM(w_out.shape, short),
            pltpu.VMEM((own, model), short),
            pltpu.VMEM((rows, width), short),
            pltpu.VMEM((NT, own, width), short),
            pltpu.VMEM((NT, own, model), short),
            pltpu.VMEM((own, model), short),
            pltpu.VMEM((NT, own, units), short),
            pltpu.VMEM((NY, 2, own, model), long),
            pltpu.VMEM((NY, own, model), short),
            pltpu.VMEM((NY, own, model), short),
            pltpu.VMEM((NY, own, model), short),
            pltpu.VMEM((NY - 1, own, model), short),
            pltpu.VMEM((2, own // 2, model), short),
            dma((2, 2, 2)),
            dma((2, 2, 4)),
            dma((2, 2, 4)),
            dma((2, 2, 2)),
            dma((2, 2, 4)),
            dma((2, 2, 4)),
            dma((2, 2, NZ)),
            dma((2, 2, NZ)),
            dma((2, 2, 4)),
            dma((2, 2, NZ)),
            dma((2, 2, NZ)),
            dma((2, NX - 1)),
            dma((2, NX - 1)),
            dma((2, 2, 2)),
            dma((6,)),
            dma((2, NT - 1)),
            dma((2, 2, 2)),
            dma((2, 5)),
            dma((2, NY)),
            dma((2, 2, 1)),
            dma((2, 2, 2)),
        ],
        compiler_params=pltpu.CompilerParams(
            vmem_limit_bytes=63 * 2**20, collective_id=0, has_side_effects=True
        ),
    )(q, k, vt, w, wd, lambdas, gain, norm_gain, residual, w_out)


def per_device(
    residual, queries, key_pairs, values, lambdas, head_gain, w_out, norm_gain, w_gate, w_up, w_down
):
    return layer(
        queries * jnp.bfloat16(HD**-0.5),
        key_pairs,
        values.T,
        jnp.concatenate([w_gate, w_up], axis=1),
        w_down.T,
        lambdas,
        head_gain[:, None],
        norm_gain[None, :],
        residual,
        w_out,
    )


def solution(mesh):
    torus = Mesh(mesh.devices.reshape(NZ, NX, NT), ("sp_0", "sp_1", "tp"))
    return jax.shard_map(
        per_device,
        mesh=torus,
        in_specs=(
            P(SP, None),
            P(SP, "tp"),
            P(SP, "tp"),
            P(SP, "tp"),
            P("tp"),
            P(),
            P(),
            P(),
            P(SP, "tp"),
            P(SP, "tp"),
            P("tp", SP),
        ),
        out_specs=P(SP_TP, None),
        check_vma=False,
    )
```

```python
import functools

import jax
import jax.numpy as jnp
from jax import lax
from jax.experimental import pallas as pl
from jax.experimental.pallas import tpu as pltpu
from jax.sharding import Mesh
from jax.sharding import PartitionSpec as P

HD = 64
SP = ("sp_0", "sp_1")
SP_TP = ("sp_0", "sp_1", "tp")
LOWEST = -1e30
EXTRA = 16
NZ = 8
NX = 4
NY = 4
NT = 8
MESH = pl.DeviceIdType.MESH


def spread_queries(q, out_ref, at):
    rows = q.shape[0]
    lane = lax.broadcasted_iota(jnp.int32, q.shape, 1)
    zero = jnp.zeros_like(q)
    q = q * jnp.asarray(HD**-0.5, q.dtype)
    out_ref[pl.ds(at, rows), :] = jnp.where(lane < HD, q, zero)
    out_ref[pl.ds(at + rows, rows), :] = jnp.where(lane >= HD, q, zero)


def attend_tile(q2, keys, values, high_ref, acc_ref):
    one_row = lax.broadcasted_iota(jnp.int32, (EXTRA, keys.shape[0]), 0) == 0
    ones = jnp.where(one_row, 1.0, 0.0).astype(values.dtype)
    values_t = jnp.concatenate([values.T, ones], axis=0)
    scores = lax.dot_general(
        keys, q2, (((1,), (1,)), ((), ())), preferred_element_type=jnp.float32
    )
    before = high_ref[...]
    after = jnp.maximum(before, jnp.max(scores, axis=0, keepdims=True))
    shrink = jnp.exp(before - after)
    weights = jnp.exp(scores - after).astype(jnp.bfloat16)
    mixed = jnp.dot(values_t, weights, preferred_element_type=jnp.float32)
    acc_ref[...] = acc_ref[...] * shrink + mixed
    high_ref[...] = after


class Ring:
    def __init__(self, target, block, send, recv, steps):
        self.target, self.block = target, block
        self.send, self.recv, self.steps = send, recv, steps

    def copy(self, way, step, at):
        src, dst = self.block(way, step, at)
        return pltpu.make_async_remote_copy(
            src_ref=src,
            dst_ref=dst,
            send_sem=self.send.at[way, step],
            recv_sem=self.recv.at[way, step],
            device_id=self.target(way),
            device_id_type=MESH,
        )

    def start(self, step):
        for way in (0, 1):
            if step < self.steps[way]:
                self.copy(way, step, 0).start()

    def arrived(self, step):
        for way in (0, 1):
            if step < self.steps[way]:
                self.copy(way, step, 1).wait_recv()

    def sent(self):
        for way in (0, 1):
            for step in range(self.steps[way]):
                self.copy(way, step, 0).wait_send()


class Gather:
    def __init__(self, rows, whole, z, x, z_target, x_target, z_sems, one_sems, two_sems):
        self.rows, self.whole, self.z, self.x = rows, whole, z, x
        self.x_target, self.one, self.two = x_target, one_sems, two_sems
        self.ring = Ring(z_target, self.z_block, z_sems.at[0], z_sems.at[1], (4, 4))

    def origin(self, index):
        step = (index + 1) // 2
        return lax.rem(self.z + (NZ - step if index % 2 else step), NZ)

    def z_block(self, way, step, at):
        half = self.rows // 2
        rows = pl.ds(0, self.rows) if step < 3 else pl.ds(half * way, half)
        origin = lax.rem(self.z + (NZ - step - at if way == 0 else step + at), NZ)
        ref = self.whole(origin, self.x, rows)
        return (ref, ref)

    def along_x(self, src, dst, sems, way, index):
        return pltpu.make_async_remote_copy(
            src_ref=src,
            dst_ref=dst,
            send_sem=sems.at[0, way, index],
            recv_sem=sems.at[1, way, index],
            device_id=self.x_target(way),
            device_id_type=MESH,
        )

    def hop(self, number, way, index, at):
        step = number - 1 + at
        from_x = lax.rem(self.x + (NX - step if way == 0 else step), NX)
        ref = self.whole(self.origin(index), from_x, pl.ds(0, self.rows))
        return self.along_x(ref, ref, self.one if number == 1 else self.two, way, index)

    def members(self, k):
        return [0] if k == 0 else [7] if k == 4 else [2 * k - 1, 2 * k]

    def second_way(self, index):
        return 0 if index in (0, 1, 3, 5) else 1

    def along_z(self, k):
        if k > 0:
            self.ring.arrived(k - 1)
        if k < 4:
            self.ring.start(k)

    def both_ways(self, k):
        for index in self.members(k):
            for way in (0, 1):
                self.hop(1, way, index, 0).start()

    def forward(self, k):
        for index in self.members(k):
            for way in (0, 1):
                self.hop(1, way, index, 1).wait_recv()
            self.hop(2, self.second_way(index), index, 0).start()

    def done(self):
        for index in range(NZ):
            self.hop(2, self.second_way(index), index, 1).wait_recv()

    def sent(self):
        self.ring.sent()
        for index in range(NZ):
            for way in (0, 1):
                self.hop(1, way, index, 0).wait_send()
            self.hop(2, self.second_way(index), index, 0).wait_send()


def layer_kernel(
    q_ref, k_ref, v_ref, wg_ref, wu_ref, wd_ref, lam_ref, gain_ref, norm_gain_ref, res_ref, wout_ref,
    out_ref,
    qb, kb, vb, q2, high, acc, osend, lsend, orecv, lrecv, orelay,
    wall, down, wout, res, heads, th, normed, hidden, units, parts, pb, pr, fs, fr, relay,
    q_sems, k_sems, v_sems, ax_sems, az_sems, bz_sems, b1_sems, b2_sems,
    cz_sems, c1_sems, c2_sems, o_sems, l_sems, or_sems, local_sems,
    h_sems, y_sems, p_sems, c_sems, r_sems, rr_sems,
):
    z, x, t = lax.axis_index("sp_0"), lax.axis_index("sp_1"), lax.axis_index("tp")
    y, core = t // 2, lax.rem(t, 2)
    rows, width = vb.shape[1:]
    wide, unit_width = wg_ref.shape
    columns = 2 * rows
    own = rows // NT

    def z_target(way):
        return {"sp_0": lax.rem(z + (1 if way == 0 else NZ - 1), NZ)}

    def x_target(way):
        return {"sp_1": lax.rem(x + (1 if way == 0 else NX - 1), NX)}

    def chip(offset):
        return lax.rem(y + offset, NY)

    def y_target(way):
        return {"tp": chip(1 if way == 0 else NY - 1) * 2 + core}

    partner = {"tp": t + 1 - 2 * core}

    def slot(way, step):
        return 0 if step == 0 else 2 * step - 1 if way == 0 else 7 if step == 4 else 2 * step

    def k_block(way, step, at):
        return (kb.at[slot(way, step + at)], kb.at[slot(way, step + 1)])

    def v_block(way, step, at):
        return (vb.at[slot(way, step + at)], vb.at[slot(way, step + 1)])

    def q_block(way, step, at):
        part = pl.ds(0, rows) if step == 0 else pl.ds(way * (rows // 2), rows // 2)
        place = lambda hops: (NX - hops if way == 0 else hops) % NX
        return (qb.at[place(step + at), part, :], qb.at[place(step + 1), part, :])

    def ax_block(way, step, at):
        part = pl.ds(0, wide) if step == 0 else pl.ds(way * (wide // 2), wide // 2)
        from_x = lax.rem(x + (NX - step - at if way == 0 else step + at), NX)
        ref = wall.at[z, from_x, part, :]
        return (ref, ref)

    def az_block(way, step, at):
        xs = pl.ds(0, NX) if step < 3 else pl.ds(0 if way == 0 else NX // 2, NX // 2)
        origin = lax.rem(z + (NZ - step - at if way == 0 else step + at), NZ)
        ref = wall.at[origin, xs, pl.ds(0, wide), :]
        return (ref, ref)

    def b_whole(from_z, from_x, part):
        return wall.at[from_z, from_x, pl.ds(wide + part.start, part.size), :]

    def c_whole(from_z, from_x, part):
        return down.at[from_z, from_x, part, :]

    def o_block(way, step, at):
        part = pl.ds(way * (width // 2), width // 2)
        if step == 0:
            return (osend.at[1, part, :], orelay.at[way])
        return (orelay.at[way], orecv.at[1, part, :])

    kring = Ring(z_target, k_block, k_sems.at[0], k_sems.at[1], (4, 3))
    vring = Ring(z_target, v_block, v_sems.at[0], v_sems.at[1], (3, 4))
    qring = Ring(x_target, q_block, q_sems.at[0], q_sems.at[1], (2, 2))
    axring = Ring(x_target, ax_block, ax_sems.at[0], ax_sems.at[1], (2, 2))
    azring = Ring(z_target, az_block, az_sems.at[0], az_sems.at[1], (4, 4))
    oring = Ring(x_target, o_block, or_sems.at[0], or_sems.at[1], (2, 2))
    later = Gather(
        wide, b_whole, z, x, z_target, x_target, bz_sems, b1_sems, b2_sems
    )
    lowest = Gather(wide, c_whole, z, x, z_target, x_target, cz_sems, c1_sems, c2_sems)

    def x_peer(g, src, dst, sems):
        return pltpu.make_async_remote_copy(
            src_ref=src,
            dst_ref=dst,
            send_sem=sems.at[0, g - 1],
            recv_sem=sems.at[1, g - 1],
            device_id={"sp_1": lax.rem(x + g, NX)},
            device_id_type=MESH,
        )

    def o_copy(g):
        return x_peer(g, osend.at[g - 1], orecv.at[g - 1], o_sems)

    def l_copy(g):
        return x_peer(g, lsend.at[g - 1], lrecv.at[g - 1], l_sems)

    locals_ = [
        pltpu.make_async_copy(src, dst, local_sems.at[i])
        for i, (src, dst) in enumerate(
            (
                (q_ref, qb.at[0]),
                (k_ref, kb.at[0]),
                (v_ref, vb.at[0]),
                (wg_ref, wall.at[z, x, pl.ds(0, wide), :]),
                (wu_ref, wall.at[z, x, pl.ds(wide, wide), :]),
                (wd_ref, down.at[z, x]),
                (res_ref.at[pl.ds(pl.multiple_of(t * own, own), own), :], res),
                (wout_ref, wout),
            )
        )
    ]
    for copy in locals_:
        copy.start()
    barrier = pltpu.get_barrier_semaphore()
    greeted = [{"sp_0": lax.rem(z + s, NZ)} for s in (1, NZ - 1)]
    greeted += [{"sp_1": lax.rem(x + s, NX)} for s in range(1, NX)]
    greeted += [{"tp": lax.rem(t + s, NT)} for s in range(1, NT)]
    for device in greeted:
        pl.semaphore_signal(barrier, inc=1, device_id=device, device_id_type=MESH)
    high[...] = jnp.full_like(high, LOWEST)
    acc[...] = jnp.zeros_like(acc)
    for copy in locals_[:6]:
        copy.wait()
    spread_queries(qb[0], q2, 0)
    pl.semaphore_wait(barrier, len(greeted))

    qring.start(0)
    kring.start(0)
    vring.start(0)
    axring.start(0)
    later.along_z(0)
    later.both_ways(0)

    def group_tile(g):
        cols = pl.ds(g * columns, columns)
        attend_tile(q2[cols, :], kb[0], vb[0], high.at[:, cols], acc.at[:, cols])

    def kv_step(s):
        kring.arrived(s)
        vring.arrived(s)
        if s < 3:
            kring.start(s + 1)
            vring.start(s + 1)

    def a_step(s):
        azring.arrived(s)
        if s < 3:
            azring.start(s + 1)

    group_tile(0)
    qring.arrived(0)
    qring.start(1)
    for g in (1, 3):
        spread_queries(qb[g], q2, g * columns)
        group_tile(g)
    axring.arrived(0)
    axring.start(1)
    kv_step(0)
    later.along_z(1)
    later.both_ways(1)
    later.forward(0)
    qring.arrived(1)
    spread_queries(qb[2], q2, 2 * columns)
    group_tile(2)

    events = {
        3: [lambda: kv_step(1)],
        4: [lambda: later.along_z(2), lambda: later.both_ways(2), lambda: later.forward(1)],
        5: [lambda: kv_step(2), lambda: axring.arrived(1), lambda: azring.start(0)],
        6: [lambda: lowest.along_z(0)],
        7: [
            lambda: kv_step(3),
            lambda: later.along_z(3),
            lambda: later.both_ways(3),
            lambda: later.forward(2),
        ],
    }

    def tile(i, carry):
        for at, todo in events.items():

            @pl.when(i == at)
            def _():
                for act in todo:
                    act()

        attend_tile(q2[...], kb[i], vb[i], high, acc)
        return carry

    lax.fori_loop(1, NZ, tile, 0)

    def result(g):
        cols = pl.ds(g * columns, columns)
        totals = acc[pl.ds(width, 1), cols]
        return acc[pl.ds(0, width), cols] / totals, high[:, cols] + jnp.log(totals)

    def stored(g):
        mix, lse = result(g)
        osend[g - 1] = mix.astype(osend.dtype)
        lsend[g - 1] = jnp.broadcast_to(lse, lsend.shape[1:])

    stored(2)
    stored(1)
    oring.start(0)
    l_copy(2).start()
    stored(3)
    o_copy(1).start()
    l_copy(1).start()
    mix, lse = result(0)
    o_copy(3).start()
    l_copy(3).start()
    later.along_z(4)
    later.both_ways(4)
    lowest.along_z(1)
    a_step(0)
    oring.arrived(0)
    oring.start(1)
    later.forward(3)
    lowest.along_z(2)
    lowest.both_ways(0)
    lowest.both_ways(1)
    for g in (1, 3):
        o_copy(g).wait_recv()
    for g in range(1, NX):
        l_copy(g).wait_recv()
    oring.arrived(1)
    lses = [lse] + [lrecv[g][:1] for g in range(NX - 1)]
    top = functools.reduce(jnp.maximum, lses)
    shares = [jnp.exp(one - top) for one in lses]
    mix = mix * shares[0]
    for g in range(NX - 1):
        mix = mix + orecv[g].astype(jnp.float32) * shares[g + 1]
    mix = mix / functools.reduce(jnp.add, shares)
    differ = mix[:, :rows] - lam_ref[0] * mix[:, rows:]
    square = jnp.mean(differ * differ, axis=0, keepdims=True)
    mine = (differ * lax.rsqrt(square + 1e-05)).T * gain_ref[...]
    heads[...] = mine.astype(heads.dtype)
    later.forward(4)

    def own_rows(index):
        return pl.ds(pl.multiple_of(index * own, own), own)

    def h_copy(d, to, home):
        return pltpu.make_async_remote_copy(
            src_ref=heads.at[own_rows(to), :],
            dst_ref=th.at[home],
            send_sem=h_sems.at[0, d - 1],
            recv_sem=h_sems.at[1, d - 1],
            device_id={"tp": to},
            device_id_type=MESH,
        )

    for d in range(1, NT):
        h_copy(d, lax.rem(t + d, NT), t).start()
    th[t] = heads[own_rows(t), :]
    a_step(1)
    lowest.along_z(3)
    lowest.both_ways(2)
    lowest.forward(0)
    for copy in locals_[6:]:
        copy.wait()
    for d in range(1, NT):
        h_copy(d, lax.rem(t + d, NT), lax.rem(t + NT - d, NT)).wait_recv()
    token_heads = jnp.concatenate([th[h] for h in range(NT)], axis=1)
    projected = jnp.dot(token_heads, wout[...], preferred_element_type=jnp.float32)
    stream = (res[...].astype(jnp.float32) + projected).astype(jnp.bfloat16)
    hidden[...] = stream
    stream = stream.astype(jnp.float32)
    scale = lax.rsqrt(jnp.mean(stream * stream, axis=-1, keepdims=True) + 1e-05)
    normed[t] = (stream * scale * norm_gain_ref[...]).astype(normed.dtype)

    def y_block(way, step, at):
        part = pl.ds(0, own) if step == 0 else pl.ds(way * (own // 2), own // 2)
        ref = normed.at[chip(NY - step - at if way == 0 else step + at) * 2 + core, part, :]
        return (ref, ref)

    yring = Ring(y_target, y_block, y_sems.at[0], y_sems.at[1], (2, 2))
    shared = ((0, 0, own), (NY - 1, 0, own), (1, 0, own), (2, 0, own // 2), (2, own // 2, own // 2))

    def p_copy(number, of_core):
        offset, first, count = shared[number]
        ref = normed.at[chip(offset) * 2 + of_core, pl.ds(first, count), :]
        return pltpu.make_async_remote_copy(
            src_ref=ref,
            dst_ref=ref,
            send_sem=p_sems.at[0, number],
            recv_sem=p_sems.at[1, number],
            device_id=partner,
            device_id_type=MESH,
        )

    yring.start(0)
    p_copy(0, core).start()
    lowest.along_z(4)
    lowest.both_ways(3)
    lowest.both_ways(4)
    lowest.forward(1)
    yring.arrived(0)
    yring.start(1)
    p_copy(1, core).start()
    p_copy(2, core).start()
    a_step(2)
    lowest.forward(2)
    yring.arrived(1)
    p_copy(3, core).start()
    p_copy(4, core).start()
    lowest.forward(3)
    lowest.forward(4)
    later.done()
    azring.arrived(3)
    for number in range(len(shared)):
        p_copy(number, 1 - core).wait_recv()
    inputs = normed[...].reshape(rows, -1)
    gate = jnp.dot(
        inputs,
        wall[:, :, :wide].reshape(-1, unit_width),
        preferred_element_type=jnp.float32,
    )
    up = jnp.dot(
        inputs,
        wall[:, :, wide:].reshape(-1, unit_width),
        preferred_element_type=jnp.float32,
    )
    gated = gate / (1.0 + jnp.exp(-gate)) * up
    units[...] = gated.astype(units.dtype).reshape(units.shape)
    lowest.done()

    def piece(offsets):
        lhs = jnp.concatenate([units[pl.ds(chip(o) * 2, 2)] for o in offsets], axis=0)
        part = lax.dot_general(
            lhs.reshape(-1, unit_width),
            down[...].reshape(-1, unit_width),
            (((1,), (1,)), ((), ())),
            preferred_element_type=jnp.float32,
        )
        part = part.reshape(len(offsets), *parts.shape[1:])
        for i, o in enumerate(offsets):
            parts[o] = part[i]
            pb[o] = parts[o, 1 - core].astype(pb.dtype)

    def pair_copy(offset):
        return pltpu.make_async_remote_copy(
            src_ref=pb.at[offset],
            dst_ref=pr.at[offset],
            send_sem=c_sems.at[0, offset],
            recv_sem=c_sems.at[1, offset],
            device_id=partner,
            device_id_type=MESH,
        )

    def paired(offset):
        pair_copy(offset).wait_recv()
        return parts[offset, core] + pr[offset].astype(jnp.float32)

    def r_block(way, step, at):
        return (fs.at[1 if way == 0 else NY - 1], fr.at[way])

    def rr_block(way, step, at):
        part = pl.ds(way * (own // 2), own // 2)
        if step == 0:
            return (fs.at[2, part, :], relay.at[way])
        return (relay.at[way], fr.at[2, part, :])

    rring = Ring(y_target, r_block, r_sems.at[0], r_sems.at[1], (1, 1))
    rrring = Ring(y_target, rr_block, rr_sems.at[0], rr_sems.at[1], (2, 2))
    piece((2, 3))
    pair_copy(2).start()
    pair_copy(3).start()
    piece((1, 0))
    pair_copy(1).start()
    pair_copy(0).start()
    fs[2] = paired(2).astype(fs.dtype)
    fs[3] = paired(3).astype(fs.dtype)
    rrring.start(0)
    fs[1] = paired(1).astype(fs.dtype)
    total = hidden[...].astype(jnp.float32) + paired(0)
    rring.start(0)
    rrring.arrived(0)
    rrring.start(1)
    rring.arrived(0)
    total = total + fr[0].astype(jnp.float32) + fr[1].astype(jnp.float32)
    rrring.arrived(1)
    out_ref[...] = (total + fr[2].astype(jnp.float32)).astype(out_ref.dtype)

    for ring in (kring, vring, qring, axring, azring, oring, later, lowest, yring, rring, rrring):
        ring.sent()
    for g in (1, 3):
        o_copy(g).wait_send()
    for g in range(1, NX):
        l_copy(g).wait_send()
    for d in range(1, NT):
        h_copy(d, lax.rem(t + d, NT), t).wait_send()
    for number in range(len(shared)):
        p_copy(number, core).wait_send()
    for offset in range(NY):
        pair_copy(offset).wait_send()


def layer(q, k, v, wg, wu, wd, lambdas, gain, norm_gain, residual, w_out):
    rows, width = v.shape
    model = residual.shape[1]
    columns = NX * 2 * rows
    own = rows // NT
    wide, units = wg.shape
    vmem = pl.BlockSpec(memory_space=pltpu.VMEM)
    smem = pl.BlockSpec(memory_space=pltpu.SMEM)
    hbm = pl.BlockSpec(memory_space=pl.ANY)
    dma = pltpu.SemaphoreType.DMA
    short, long = jnp.bfloat16, jnp.float32
    return pl.pallas_call(
        layer_kernel,
        out_shape=jax.ShapeDtypeStruct((own, model), short),
        in_specs=[hbm] * 6 + [smem, vmem, vmem, hbm, hbm],
        out_specs=vmem,
        scratch_shapes=[
            pltpu.VMEM((NX, rows, 2 * HD), short),
            pltpu.VMEM((NZ, rows, 2 * HD), short),
            pltpu.VMEM((NZ, rows, width), short),
            pltpu.VMEM((columns, 2 * HD), short),
            pltpu.VMEM((1, columns), long),
            pltpu.VMEM((width + EXTRA, columns), long),
            pltpu.VMEM((NX - 1, width, 2 * rows), short),
            pltpu.VMEM((NX - 1, 8, 2 * rows), long),
            pltpu.VMEM((NX - 1, width, 2 * rows), short),
            pltpu.VMEM((NX - 1, 8, 2 * rows), long),
            pltpu.VMEM((2, width // 2, 2 * rows), short),
            pltpu.VMEM((NZ, NX, 2 * wide, units), short),
            pltpu.VMEM((NZ, NX, *wd.shape), short),
            pltpu.VMEM(w_out.shape, short),
            pltpu.VMEM((own, model), short),
            pltpu.VMEM((rows, width), short),
            pltpu.VMEM((NT, own, width), short),
            pltpu.VMEM((NT, own, model), short),
            pltpu.VMEM((own, model), short),
            pltpu.VMEM((NT, own, units), short),
            pltpu.VMEM((NY, 2, own, model), long),
            pltpu.VMEM((NY, own, model), short),
            pltpu.VMEM((NY, own, model), short),
            pltpu.VMEM((NY, own, model), short),
            pltpu.VMEM((NY - 1, own, model), short),
            pltpu.VMEM((2, own // 2, model), short),
            dma((2, 2, 2)),
            dma((2, 2, 4)),
            dma((2, 2, 4)),
            dma((2, 2, 2)),
            dma((2, 2, 4)),
            dma((2, 2, 4)),
            dma((2, 2, NZ)),
            dma((2, 2, NZ)),
            dma((2, 2, 4)),
            dma((2, 2, NZ)),
            dma((2, 2, NZ)),
            dma((2, NX - 1)),
            dma((2, NX - 1)),
            dma((2, 2, 2)),
            dma((8,)),
            dma((2, NT - 1)),
            dma((2, 2, 2)),
            dma((2, 5)),
            dma((2, NY)),
            dma((2, 2, 1)),
            dma((2, 2, 2)),
        ],
        compiler_params=pltpu.CompilerParams(
            vmem_limit_bytes=63 * 2**20, collective_id=0, has_side_effects=True
        ),
    )(q, k, v, wg, wu, wd, lambdas, gain, norm_gain, residual, w_out)


def per_device(
    residual, queries, key_pairs, values, lambdas, head_gain, w_out, norm_gain, w_gate, w_up, w_down
):
    return layer(
        queries,
        key_pairs,
        values,
        w_gate,
        w_up,
        w_down.T,
        lambdas,
        head_gain[None, :],
        norm_gain[None, :],
        residual,
        w_out,
    )


def solution(mesh):
    torus = Mesh(mesh.devices.reshape(NZ, NX, NT), ("sp_0", "sp_1", "tp"))
    return jax.shard_map(
        per_device,
        mesh=torus,
        in_specs=(
            P(SP, None),
            P(SP, "tp"),
            P(SP, "tp"),
            P(SP, "tp"),
            P("tp"),
            P(),
            P(),
            P(),
            P(SP, "tp"),
            P(SP, "tp"),
            P("tp", SP),
        ),
        out_specs=P(SP_TP, None),
        check_vma=False,
    )
```

```python
import functools

import jax
import jax.numpy as jnp
from jax import lax
from jax.experimental import pallas as pl
from jax.experimental.pallas import tpu as pltpu
from jax.sharding import Mesh
from jax.sharding import PartitionSpec as P

HD = 64
SP = ("sp_0", "sp_1")
SP_TP = ("sp_0", "sp_1", "tp")
LOWEST = -1e30
EXTRA = 16
SPLIT = 5
NZ = 8
NX = 4
NY = 4
NT = 8
MESH = pl.DeviceIdType.MESH


def spread_queries(q, out_ref, at):
    rows = q.shape[0]
    lane = lax.broadcasted_iota(jnp.int32, q.shape, 1)
    zero = jnp.zeros_like(q)
    q = q * jnp.asarray(HD**-0.5, q.dtype)
    out_ref[pl.ds(at, rows), :] = jnp.where(lane < HD, q, zero)
    out_ref[pl.ds(at + rows, rows), :] = jnp.where(lane >= HD, q, zero)


def attend_tile(q2, keys, values, high_ref, acc_ref):
    one_row = lax.broadcasted_iota(jnp.int32, (EXTRA, keys.shape[0]), 0) == 0
    ones = jnp.where(one_row, 1.0, 0.0).astype(values.dtype)
    values_t = jnp.concatenate([values.T, ones], axis=0)
    scores = lax.dot_general(
        keys, q2, (((1,), (1,)), ((), ())), preferred_element_type=jnp.float32
    )
    before = high_ref[...]
    after = jnp.maximum(before, jnp.max(scores, axis=0, keepdims=True))
    shrink = jnp.exp(before - after)
    weights = jnp.exp(scores - after).astype(jnp.bfloat16)
    mixed = jnp.dot(values_t, weights, preferred_element_type=jnp.float32)
    acc_ref[...] = acc_ref[...] * shrink + mixed
    high_ref[...] = after


class Ring:
    def __init__(self, target, block, send, recv, steps):
        self.target, self.block = target, block
        self.send, self.recv, self.steps = send, recv, steps

    def copy(self, way, step, at):
        src, dst = self.block(way, step, at)
        return pltpu.make_async_remote_copy(
            src_ref=src,
            dst_ref=dst,
            send_sem=self.send.at[way, step],
            recv_sem=self.recv.at[way, step],
            device_id=self.target(way),
            device_id_type=MESH,
        )

    def start(self, step):
        for way in (0, 1):
            if step < self.steps[way]:
                self.copy(way, step, 0).start()

    def arrived(self, step):
        for way in (0, 1):
            if step < self.steps[way]:
                self.copy(way, step, 1).wait_recv()

    def sent(self):
        for way in (0, 1):
            for step in range(self.steps[way]):
                self.copy(way, step, 0).wait_send()


class Gather:
    def __init__(self, rows, whole, z, x, z_target, x_target, z_sems, one_sems, two_sems):
        self.rows, self.whole, self.z, self.x = rows, whole, z, x
        self.x_target, self.one, self.two = x_target, one_sems, two_sems
        self.ring = Ring(z_target, self.z_block, z_sems.at[0], z_sems.at[1], (4, 4))

    def origin(self, index):
        step = (index + 1) // 2
        return lax.rem(self.z + (NZ - step if index % 2 else step), NZ)

    def z_block(self, way, step, at):
        half = self.rows // 2
        rows = pl.ds(0, self.rows) if step < 3 else pl.ds(half * way, half)
        origin = lax.rem(self.z + (NZ - step - at if way == 0 else step + at), NZ)
        ref = self.whole(origin, self.x, rows)
        return (ref, ref)

    def along_x(self, src, dst, sems, way, index):
        return pltpu.make_async_remote_copy(
            src_ref=src,
            dst_ref=dst,
            send_sem=sems.at[0, way, index],
            recv_sem=sems.at[1, way, index],
            device_id=self.x_target(way),
            device_id_type=MESH,
        )

    def hop(self, number, way, index, at):
        step = number - 1 + at
        from_x = lax.rem(self.x + (NX - step if way == 0 else step), NX)
        ref = self.whole(self.origin(index), from_x, pl.ds(0, self.rows))
        return self.along_x(ref, ref, self.one if number == 1 else self.two, way, index)

    def members(self, k):
        return [0] if k == 0 else [7] if k == 4 else [2 * k - 1, 2 * k]

    def second_way(self, index):
        return 0 if index in (0, 1, 3, 5) else 1

    def along_z(self, k):
        if k > 0:
            self.ring.arrived(k - 1)
        if k < 4:
            self.ring.start(k)

    def both_ways(self, k):
        for index in self.members(k):
            for way in (0, 1):
                self.hop(1, way, index, 0).start()

    def forward(self, k):
        for index in self.members(k):
            for way in (0, 1):
                self.hop(1, way, index, 1).wait_recv()
            self.hop(2, self.second_way(index), index, 0).start()

    def done(self):
        for index in range(NZ):
            self.hop(2, self.second_way(index), index, 1).wait_recv()

    def sent(self):
        self.ring.sent()
        for index in range(NZ):
            for way in (0, 1):
                self.hop(1, way, index, 0).wait_send()
            self.hop(2, self.second_way(index), index, 0).wait_send()


def layer_kernel(
    q_ref, k_ref, v_ref, wg_ref, wu_ref, wd_ref, lam_ref, gain_ref, norm_gain_ref, res_ref, wout_ref,
    out_ref,
    qb, kb, vb, q2, high, acc, osend, lsend, orecv, lrecv, orelay,
    wall, down, wout, res, heads, th, normed, hidden, units, parts, pb, pr, fs, fr, relay,
    q_sems, k_sems, v_sems, ax_sems, az_sems, bz_sems, b1_sems, b2_sems,
    cz_sems, c1_sems, c2_sems, o_sems, l_sems, or_sems, local_sems,
    h_sems, y_sems, p_sems, c_sems, r_sems, rr_sems, gate_own, up_own,
):
    z, x, t = lax.axis_index("sp_0"), lax.axis_index("sp_1"), lax.axis_index("tp")
    y, core = t // 2, lax.rem(t, 2)
    rows, width = vb.shape[1:]
    wide, unit_width = wg_ref.shape
    half = wide // 2
    columns = 2 * rows
    own = rows // NT

    def z_target(way):
        return {"sp_0": lax.rem(z + (1 if way == 0 else NZ - 1), NZ)}

    def x_target(way):
        return {"sp_1": lax.rem(x + (1 if way == 0 else NX - 1), NX)}

    def chip(offset):
        return lax.rem(y + offset, NY)

    def y_target(way):
        return {"tp": chip(1 if way == 0 else NY - 1) * 2 + core}

    partner = {"tp": t + 1 - 2 * core}

    def slot(way, step):
        return 0 if step == 0 else 2 * step - 1 if way == 0 else 7 if step == 4 else 2 * step

    def k_block(way, step, at):
        return (kb.at[slot(way, step + at)], kb.at[slot(way, step + 1)])

    def v_block(way, step, at):
        return (vb.at[slot(way, step + at)], vb.at[slot(way, step + 1)])

    def q_block(way, step, at):
        part = pl.ds(0, rows) if step == 0 else pl.ds(way * (rows // 2), rows // 2)
        place = lambda hops: (NX - hops if way == 0 else hops) % NX
        return (qb.at[place(step + at), part, :], qb.at[place(step + 1), part, :])

    def ax_block(way, step, at):
        part = pl.ds(0, half) if step == 0 else pl.ds(way * (half // 2), half // 2)
        from_x = lax.rem(x + (NX - step - at if way == 0 else step + at), NX)
        ref = wall.at[z, from_x, part, :]
        return (ref, ref)

    def az_block(way, step, at):
        xs = pl.ds(0, NX) if step < 3 else pl.ds(0 if way == 0 else NX // 2, NX // 2)
        origin = lax.rem(z + (NZ - step - at if way == 0 else step + at), NZ)
        ref = wall.at[origin, xs, pl.ds(0, half), :]
        return (ref, ref)

    def b_whole(from_z, from_x, part):
        return wall.at[from_z, from_x, pl.ds(half + part.start, part.size), :]

    def c_whole(from_z, from_x, part):
        return down.at[from_z, from_x, part, :]

    def o_block(way, step, at):
        part = pl.ds(way * (width // 2), width // 2)
        if step == 0:
            return (osend.at[1, part, :], orelay.at[way])
        return (orelay.at[way], orecv.at[1, part, :])

    kring = Ring(z_target, k_block, k_sems.at[0], k_sems.at[1], (4, 3))
    vring = Ring(z_target, v_block, v_sems.at[0], v_sems.at[1], (3, 4))
    qring = Ring(x_target, q_block, q_sems.at[0], q_sems.at[1], (2, 2))
    axring = Ring(x_target, ax_block, ax_sems.at[0], ax_sems.at[1], (2, 2))
    azring = Ring(z_target, az_block, az_sems.at[0], az_sems.at[1], (4, 4))
    oring = Ring(x_target, o_block, or_sems.at[0], or_sems.at[1], (2, 2))
    later = Gather(
        half, b_whole, z, x, z_target, x_target, bz_sems, b1_sems, b2_sems
    )
    lowest = Gather(wide, c_whole, z, x, z_target, x_target, cz_sems, c1_sems, c2_sems)

    def x_peer(g, src, dst, sems):
        return pltpu.make_async_remote_copy(
            src_ref=src,
            dst_ref=dst,
            send_sem=sems.at[0, g - 1],
            recv_sem=sems.at[1, g - 1],
            device_id={"sp_1": lax.rem(x + g, NX)},
            device_id_type=MESH,
        )

    def o_copy(g):
        return x_peer(g, osend.at[g - 1], orecv.at[g - 1], o_sems)

    def l_copy(g):
        return x_peer(g, lsend.at[g - 1], lrecv.at[g - 1], l_sems)

    locals_ = [
        pltpu.make_async_copy(src, dst, local_sems.at[i])
        for i, (src, dst) in enumerate(
            (
                (q_ref, qb.at[0]),
                (k_ref, kb.at[0]),
                (v_ref, vb.at[0]),
                (wg_ref, gate_own),
                (wu_ref, up_own),
                (wd_ref, down.at[z, x]),
                (res_ref.at[pl.ds(pl.multiple_of(t * own, own), own), :], res),
                (wout_ref, wout),
            )
        )
    ]
    for copy in locals_:
        copy.start()
    barrier = pltpu.get_barrier_semaphore()
    greeted = [{"sp_0": lax.rem(z + s, NZ)} for s in (1, NZ - 1)]
    greeted += [{"sp_1": lax.rem(x + s, NX)} for s in range(1, NX)]
    greeted += [{"tp": lax.rem(t + s, NT)} for s in range(1, NT)]
    for device in greeted:
        pl.semaphore_signal(barrier, inc=1, device_id=device, device_id_type=MESH)
    high[...] = jnp.full_like(high, LOWEST)
    acc[...] = jnp.zeros_like(acc)
    for copy in locals_[:6]:
        copy.wait()
    wall[z, x] = jnp.concatenate([gate_own[...], up_own[...]], axis=1)
    spread_queries(qb[0], q2, 0)
    pl.semaphore_wait(barrier, len(greeted))

    qring.start(0)
    kring.start(0)
    vring.start(0)
    axring.start(0)
    later.along_z(0)

    def group_tile(g):
        cols = pl.ds(g * columns, columns)
        attend_tile(q2[cols, :], kb[0], vb[0], high.at[:, cols], acc.at[:, cols])

    def kv_step(s):
        kring.arrived(s)
        vring.arrived(s)
        if s < 3:
            kring.start(s + 1)
            vring.start(s + 1)

    def a_step(s):
        azring.arrived(s)
        if s < 3:
            azring.start(s + 1)

    group_tile(0)
    qring.arrived(0)
    qring.start(1)
    later.both_ways(0)
    kv_step(0)
    axring.arrived(0)
    axring.start(1)
    for g in (1, 3):
        spread_queries(qb[g], q2, g * columns)
        group_tile(g)
    qring.arrived(1)
    spread_queries(qb[2], q2, 2 * columns)
    group_tile(2)

    def weight_step(gather, k):
        gather.along_z(k)
        gather.both_ways(k)

    events = {
        1: [lambda: weight_step(later, 1), lambda: later.forward(0)],
        2: [lambda: kv_step(1)],
        3: [lambda: weight_step(later, 2), lambda: later.forward(1), lambda: weight_step(lowest, 0)],
        4: [lambda: kv_step(2), lambda: axring.arrived(1), lambda: azring.start(0)],
    }

    def tile(i, carry):
        for at, todo in events.items():

            @pl.when(i == at)
            def _():
                for act in todo:
                    act()

        attend_tile(q2[...], kb[i], vb[i], high, acc)
        return carry

    lax.fori_loop(1, SPLIT, tile, 0)

    def last_tile(g):
        cols = pl.ds(g * columns, columns)
        keys = kb[SPLIT:].reshape(-1, kb.shape[-1])
        values = vb[SPLIT:].reshape(-1, vb.shape[-1])
        attend_tile(q2[cols, :], keys, values, high.at[:, cols], acc.at[:, cols])

    def result(g):
        cols = pl.ds(g * columns, columns)
        totals = acc[pl.ds(width, 1), cols]
        return acc[pl.ds(0, width), cols] / totals, high[:, cols] + jnp.log(totals)

    def stored(g):
        mix, lse = result(g)
        osend[g - 1] = mix.astype(osend.dtype)
        lsend[g - 1] = jnp.broadcast_to(lse, lsend.shape[1:])

    weight_step(later, 3)
    later.forward(2)
    kv_step(3)
    last_tile(2)
    stored(2)
    oring.start(0)
    l_copy(2).start()
    last_tile(1)
    stored(1)
    lowest.along_z(1)
    o_copy(1).start()
    l_copy(1).start()
    last_tile(3)
    stored(3)
    oring.arrived(0)
    oring.start(1)
    o_copy(3).start()
    l_copy(3).start()
    lowest.along_z(2)
    a_step(0)
    last_tile(0)
    mix, lse = result(0)
    lowest.both_ways(1)
    later.along_z(4)
    later.both_ways(4)
    later.forward(3)
    lowest.forward(0)
    lowest.along_z(3)
    for g in (1, 3):
        o_copy(g).wait_recv()
    for g in range(1, NX):
        l_copy(g).wait_recv()
    oring.arrived(1)
    lses = [lse] + [lrecv[g][:1] for g in range(NX - 1)]
    top = functools.reduce(jnp.maximum, lses)
    shares = [jnp.exp(one - top) for one in lses]
    mix = mix * shares[0]
    for g in range(NX - 1):
        mix = mix + orecv[g].astype(jnp.float32) * shares[g + 1]
    mix = mix / functools.reduce(jnp.add, shares)
    differ = mix[:, :rows] - lam_ref[0] * mix[:, rows:]
    square = jnp.mean(differ * differ, axis=0, keepdims=True)
    mine = (differ * lax.rsqrt(square + 1e-05)).T * gain_ref[...]
    heads[...] = mine.astype(heads.dtype)

    def own_rows(index):
        return pl.ds(pl.multiple_of(index * own, own), own)

    def h_copy(d, to, home):
        return pltpu.make_async_remote_copy(
            src_ref=heads.at[own_rows(to), :],
            dst_ref=th.at[home],
            send_sem=h_sems.at[0, d - 1],
            recv_sem=h_sems.at[1, d - 1],
            device_id={"tp": to},
            device_id_type=MESH,
        )

    for d in range(1, NT):
        h_copy(d, lax.rem(t + d, NT), t).start()
    th[t] = heads[own_rows(t), :]
    a_step(1)
    lowest.both_ways(2)
    lowest.both_ways(3)
    for copy in locals_[6:]:
        copy.wait()
    for d in range(1, NT):
        h_copy(d, lax.rem(t + d, NT), lax.rem(t + NT - d, NT)).wait_recv()
    token_heads = jnp.concatenate([th[h] for h in range(NT)], axis=1)
    projected = jnp.dot(token_heads, wout[...], preferred_element_type=jnp.float32)
    stream = (res[...].astype(jnp.float32) + projected).astype(jnp.bfloat16)
    hidden[...] = stream
    stream = stream.astype(jnp.float32)
    scale = lax.rsqrt(jnp.mean(stream * stream, axis=-1, keepdims=True) + 1e-05)
    normed[t] = (stream * scale * norm_gain_ref[...]).astype(normed.dtype)

    def y_block(way, step, at):
        part = pl.ds((1 - way if step == 1 else way) * (own // 2), own // 2)
        hops = step // 2 + at
        ref = normed.at[chip(NY - hops if way == 0 else hops) * 2 + core, part, :]
        return (ref, ref)

    yring = Ring(y_target, y_block, y_sems.at[0], y_sems.at[1], (3, 3))
    shared = ((0, 0, own), (NY - 1, 0, own), (1, 0, own), (2, 0, own // 2), (2, own // 2, own // 2))

    def p_copy(number, of_core):
        offset, first, count = shared[number]
        ref = normed.at[chip(offset) * 2 + of_core, pl.ds(first, count), :]
        return pltpu.make_async_remote_copy(
            src_ref=ref,
            dst_ref=ref,
            send_sem=p_sems.at[0, number],
            recv_sem=p_sems.at[1, number],
            device_id=partner,
            device_id_type=MESH,
        )

    yring.start(0)
    yring.start(1)
    p_copy(0, core).start()
    weight_step(lowest, 4)
    later.forward(4)
    lowest.forward(1)
    yring.arrived(0)
    yring.start(2)
    a_step(2)
    yring.arrived(1)
    p_copy(1, core).start()
    p_copy(2, core).start()
    lowest.forward(2)
    lowest.forward(3)
    yring.arrived(2)
    p_copy(3, core).start()
    p_copy(4, core).start()
    later.done()
    azring.arrived(3)
    lowest.forward(4)
    for number in range(len(shared)):
        p_copy(number, 1 - core).wait_recv()
    inputs = normed[...].reshape(rows, -1)
    both = wall[...].reshape(-1, wall.shape[-1])
    sums = jnp.dot(inputs, both, preferred_element_type=jnp.float32)
    gate, up = sums[:, :unit_width], sums[:, unit_width:]
    gated = gate / (1.0 + jnp.exp(-gate)) * up
    units[...] = gated.astype(units.dtype).reshape(units.shape)
    lowest.done()

    def piece(offsets):
        lhs = jnp.concatenate([units[pl.ds(chip(o) * 2, 2)] for o in offsets], axis=0)
        part = lax.dot_general(
            lhs.reshape(-1, unit_width),
            down[...].reshape(-1, unit_width),
            (((1,), (1,)), ((), ())),
            preferred_element_type=jnp.float32,
        )
        part = part.reshape(len(offsets), *parts.shape[1:])
        for i, o in enumerate(offsets):
            parts[o] = part[i]
            pb[o] = parts[o, 1 - core].astype(pb.dtype)

    def pair_copy(offset):
        return pltpu.make_async_remote_copy(
            src_ref=pb.at[offset],
            dst_ref=pr.at[offset],
            send_sem=c_sems.at[0, offset],
            recv_sem=c_sems.at[1, offset],
            device_id=partner,
            device_id_type=MESH,
        )

    def paired(offset):
        pair_copy(offset).wait_recv()
        return parts[offset, core] + pr[offset].astype(jnp.float32)

    def r_block(way, step, at):
        part = pl.ds((way if step == 1 else 1 - way) * (own // 2), own // 2)
        return (fs.at[1 if way == 0 else NY - 1, part, :], fr.at[way, part, :])

    def rr_block(way, step, at):
        return (fs.at[2, pl.ds(way * (own // 2), own // 2), :], relay.at[way])

    rring = Ring(y_target, r_block, r_sems.at[0], r_sems.at[1], (2, 2))
    rrring = Ring(y_target, rr_block, rr_sems.at[0], rr_sems.at[1], (1, 1))
    piece((2, 3))
    pair_copy(2).start()
    pair_copy(3).start()
    piece((1, 0))
    pair_copy(1).start()
    pair_copy(0).start()
    fs[2] = paired(2).astype(fs.dtype)
    rrring.start(0)
    ahead = paired(1)
    fs[1, own // 2 :] = ahead[own // 2 :].astype(fs.dtype)
    behind = paired(3)
    fs[3, : own // 2] = behind[: own // 2].astype(fs.dtype)
    rring.start(0)
    total = hidden[...].astype(jnp.float32) + paired(0)
    rrring.arrived(0)
    fs[1, : own // 2] = (ahead[: own // 2] + relay[0].astype(jnp.float32)).astype(fs.dtype)
    fs[3, own // 2 :] = (behind[own // 2 :] + relay[1].astype(jnp.float32)).astype(fs.dtype)
    rring.start(1)
    rring.arrived(0)
    rring.arrived(1)
    total = total + fr[0].astype(jnp.float32) + fr[1].astype(jnp.float32)
    out_ref[...] = total.astype(out_ref.dtype)

    for ring in (kring, vring, qring, axring, azring, oring, later, lowest, yring, rring, rrring):
        ring.sent()
    for g in (1, 3):
        o_copy(g).wait_send()
    for g in range(1, NX):
        l_copy(g).wait_send()
    for d in range(1, NT):
        h_copy(d, lax.rem(t + d, NT), t).wait_send()
    for number in range(len(shared)):
        p_copy(number, core).wait_send()
    for offset in range(NY):
        pair_copy(offset).wait_send()


def layer(q, k, v, wg, wu, wd, lambdas, gain, norm_gain, residual, w_out):
    rows, width = v.shape
    model = residual.shape[1]
    columns = NX * 2 * rows
    own = rows // NT
    wide, units = wg.shape
    vmem = pl.BlockSpec(memory_space=pltpu.VMEM)
    smem = pl.BlockSpec(memory_space=pltpu.SMEM)
    hbm = pl.BlockSpec(memory_space=pl.ANY)
    dma = pltpu.SemaphoreType.DMA
    short, long = jnp.bfloat16, jnp.float32
    return pl.pallas_call(
        layer_kernel,
        out_shape=jax.ShapeDtypeStruct((own, model), short),
        in_specs=[hbm] * 6 + [smem, vmem, vmem, hbm, hbm],
        out_specs=vmem,
        scratch_shapes=[
            pltpu.VMEM((NX, rows, 2 * HD), short),
            pltpu.VMEM((NZ, rows, 2 * HD), short),
            pltpu.VMEM((NZ, rows, width), short),
            pltpu.VMEM((columns, 2 * HD), short),
            pltpu.VMEM((1, columns), long),
            pltpu.VMEM((width + EXTRA, columns), long),
            pltpu.VMEM((NX - 1, width, 2 * rows), short),
            pltpu.VMEM((NX - 1, 8, 2 * rows), long),
            pltpu.VMEM((NX - 1, width, 2 * rows), short),
            pltpu.VMEM((NX - 1, 8, 2 * rows), long),
            pltpu.VMEM((2, width // 2, 2 * rows), short),
            pltpu.VMEM((NZ, NX, wide, 2 * units), short),
            pltpu.VMEM((NZ, NX, *wd.shape), short),
            pltpu.VMEM(w_out.shape, short),
            pltpu.VMEM((own, model), short),
            pltpu.VMEM((rows, width), short),
            pltpu.VMEM((NT, own, width), short),
            pltpu.VMEM((NT, own, model), short),
            pltpu.VMEM((own, model), short),
            pltpu.VMEM((NT, own, units), short),
            pltpu.VMEM((NY, 2, own, model), long),
            pltpu.VMEM((NY, own, model), short),
            pltpu.VMEM((NY, own, model), short),
            pltpu.VMEM((NY, own, model), short),
            pltpu.VMEM((2, own, model), short),
            pltpu.VMEM((2, own // 2, model), short),
            dma((2, 2, 2)),
            dma((2, 2, 4)),
            dma((2, 2, 4)),
            dma((2, 2, 2)),
            dma((2, 2, 4)),
            dma((2, 2, 4)),
            dma((2, 2, NZ)),
            dma((2, 2, NZ)),
            dma((2, 2, 4)),
            dma((2, 2, NZ)),
            dma((2, 2, NZ)),
            dma((2, NX - 1)),
            dma((2, NX - 1)),
            dma((2, 2, 2)),
            dma((8,)),
            dma((2, NT - 1)),
            dma((2, 2, 3)),
            dma((2, 5)),
            dma((2, NY)),
            dma((2, 2, 2)),
            dma((2, 2, 1)),
            pltpu.VMEM((wide, units), short),
            pltpu.VMEM((wide, units), short),
        ],
        compiler_params=pltpu.CompilerParams(
            vmem_limit_bytes=63 * 2**20, collective_id=0, has_side_effects=True
        ),
    )(q, k, v, wg, wu, wd, lambdas, gain, norm_gain, residual, w_out)


def per_device(
    residual, queries, key_pairs, values, lambdas, head_gain, w_out, norm_gain, w_gate, w_up, w_down
):
    return layer(
        queries,
        key_pairs,
        values,
        w_gate,
        w_up,
        w_down.T,
        lambdas,
        head_gain[None, :],
        norm_gain[None, :],
        residual,
        w_out,
    )


def solution(mesh):
    torus = Mesh(mesh.devices.reshape(NZ, NX, NT), ("sp_0", "sp_1", "tp"))
    return jax.shard_map(
        per_device,
        mesh=torus,
        in_specs=(
            P(SP, None),
            P(SP, "tp"),
            P(SP, "tp"),
            P(SP, "tp"),
            P("tp"),
            P(),
            P(),
            P(),
            P(SP, "tp"),
            P(SP, "tp"),
            P("tp", SP),
        ),
        out_specs=P(SP_TP, None),
        check_vma=False,
    )
```

```python
import functools

import jax
import jax.numpy as jnp
from jax import lax
from jax.experimental import pallas as pl
from jax.experimental.pallas import tpu as pltpu
from jax.sharding import Mesh
from jax.sharding import PartitionSpec as P

HD = 64
SP = ("sp_0", "sp_1")
SP_TP = ("sp_0", "sp_1", "tp")
LOWEST = -1e30
EXTRA = 16
SPLIT = 5
NZ = 8
NX = 4
NY = 4
NT = 8
MESH = pl.DeviceIdType.MESH


def spread_queries(q, out_ref, at):
    rows = q.shape[0]
    lane = lax.broadcasted_iota(jnp.int32, q.shape, 1)
    zero = jnp.zeros_like(q)
    q = q * jnp.asarray(HD**-0.5, q.dtype)
    out_ref[pl.ds(at, rows), :] = jnp.where(lane < HD, q, zero)
    out_ref[pl.ds(at + rows, rows), :] = jnp.where(lane >= HD, q, zero)


def attend_tile(q2, keys, values, high_ref, acc_ref):
    one_row = lax.broadcasted_iota(jnp.int32, (EXTRA, keys.shape[0]), 0) == 0
    ones = jnp.where(one_row, 1.0, 0.0).astype(values.dtype)
    values_t = jnp.concatenate([values.T, ones], axis=0)
    scores = lax.dot_general(
        keys, q2, (((1,), (1,)), ((), ())), preferred_element_type=jnp.float32
    )
    before = high_ref[...]
    after = jnp.maximum(before, jnp.max(scores, axis=0, keepdims=True))
    shrink = jnp.exp(before - after)
    weights = jnp.exp(scores - after).astype(jnp.bfloat16)
    mixed = jnp.dot(values_t, weights, preferred_element_type=jnp.float32)
    acc_ref[...] = acc_ref[...] * shrink + mixed
    high_ref[...] = after


class Ring:
    def __init__(self, target, block, send, recv, steps):
        self.target, self.block = target, block
        self.send, self.recv, self.steps = send, recv, steps

    def copy(self, way, step, at):
        src, dst = self.block(way, step, at)
        return pltpu.make_async_remote_copy(
            src_ref=src,
            dst_ref=dst,
            send_sem=self.send.at[way, step],
            recv_sem=self.recv.at[way, step],
            device_id=self.target(way),
            device_id_type=MESH,
        )

    def start(self, step):
        for way in (0, 1):
            if step < self.steps[way]:
                self.copy(way, step, 0).start()

    def arrived(self, step):
        for way in (0, 1):
            if step < self.steps[way]:
                self.copy(way, step, 1).wait_recv()

    def sent(self):
        for way in (0, 1):
            for step in range(self.steps[way]):
                self.copy(way, step, 0).wait_send()


class Gather:
    def __init__(self, rows, whole, z, x, z_target, x_target, z_sems, one_sems, two_sems):
        self.rows, self.whole, self.z, self.x = rows, whole, z, x
        self.x_target, self.one, self.two = x_target, one_sems, two_sems
        self.ring = Ring(z_target, self.z_block, z_sems.at[0], z_sems.at[1], (4, 4))

    def origin(self, index):
        step = (index + 1) // 2
        return lax.rem(self.z + (NZ - step if index % 2 else step), NZ)

    def z_block(self, way, step, at):
        half = self.rows // 2
        rows = pl.ds(0, self.rows) if step < 3 else pl.ds(half * way, half)
        origin = lax.rem(self.z + (NZ - step - at if way == 0 else step + at), NZ)
        ref = self.whole(origin, self.x, rows)
        return (ref, ref)

    def along_x(self, src, dst, sems, way, index):
        return pltpu.make_async_remote_copy(
            src_ref=src,
            dst_ref=dst,
            send_sem=sems.at[0, way, index],
            recv_sem=sems.at[1, way, index],
            device_id=self.x_target(way),
            device_id_type=MESH,
        )

    def hop(self, number, way, index, at):
        step = number - 1 + at
        from_x = lax.rem(self.x + (NX - step if way == 0 else step), NX)
        ref = self.whole(self.origin(index), from_x, pl.ds(0, self.rows))
        return self.along_x(ref, ref, self.one if number == 1 else self.two, way, index)

    def members(self, k):
        return [0] if k == 0 else [7] if k == 4 else [2 * k - 1, 2 * k]

    def second_way(self, index):
        return 0 if index in (0, 1, 3, 5) else 1

    def along_z(self, k):
        if k > 0:
            self.ring.arrived(k - 1)
        if k < 4:
            self.ring.start(k)

    def both_ways(self, k):
        for index in self.members(k):
            for way in (0, 1):
                self.hop(1, way, index, 0).start()

    def forward(self, k):
        for index in self.members(k):
            for way in (0, 1):
                self.hop(1, way, index, 1).wait_recv()
            self.hop(2, self.second_way(index), index, 0).start()

    def done(self):
        for index in range(NZ):
            self.hop(2, self.second_way(index), index, 1).wait_recv()

    def sent(self):
        self.ring.sent()
        for index in range(NZ):
            for way in (0, 1):
                self.hop(1, way, index, 0).wait_send()
            self.hop(2, self.second_way(index), index, 0).wait_send()


def layer_kernel(
    q_ref, k_ref, v_ref, wg_ref, wu_ref, wd_ref, lam_ref, gain_ref, norm_gain_ref, res_ref, wout_ref,
    out_ref,
    qb, kb, vb, q2, high, acc, osend, lsend, orecv, lrecv, orelay,
    wall, down, wout, res, heads, th, normed, hidden, units, parts, pb, pr, fs, fr, relay,
    q_sems, k_sems, v_sems, ax_sems, az_sems, bz_sems, b1_sems, b2_sems,
    cz_sems, c1_sems, c2_sems, o_sems, l_sems, or_sems, local_sems,
    h_sems, y_sems, p_sems, c_sems, r_sems, rr_sems, gate_own, up_own,
    lrelay, lr_sems,
):
    z, x, t = lax.axis_index("sp_0"), lax.axis_index("sp_1"), lax.axis_index("tp")
    y, core = t // 2, lax.rem(t, 2)
    rows, width = vb.shape[1:]
    wide, unit_width = wg_ref.shape
    half = wide // 2
    columns = 2 * rows
    own = rows // NT

    def z_target(way):
        return {"sp_0": lax.rem(z + (1 if way == 0 else NZ - 1), NZ)}

    def x_target(way):
        return {"sp_1": lax.rem(x + (1 if way == 0 else NX - 1), NX)}

    def chip(offset):
        return lax.rem(y + offset, NY)

    def y_target(way):
        return {"tp": chip(1 if way == 0 else NY - 1) * 2 + core}

    partner = {"tp": t + 1 - 2 * core}

    def slot(way, step):
        return 0 if step == 0 else 2 * step - 1 if way == 0 else 7 if step == 4 else 2 * step

    def k_block(way, step, at):
        return (kb.at[slot(way, step + at)], kb.at[slot(way, step + 1)])

    def v_block(way, step, at):
        return (vb.at[slot(way, step + at)], vb.at[slot(way, step + 1)])

    def q_block(way, step, at):
        part = pl.ds(0, rows) if step == 0 else pl.ds(way * (rows // 2), rows // 2)
        place = lambda hops: (NX - hops if way == 0 else hops) % NX
        return (qb.at[place(step + at), part, :], qb.at[place(step + 1), part, :])

    def ax_block(way, step, at):
        part = pl.ds(0, half) if step == 0 else pl.ds(way * (half // 2), half // 2)
        from_x = lax.rem(x + (NX - step - at if way == 0 else step + at), NX)
        ref = wall.at[z, from_x, part, :]
        return (ref, ref)

    def az_block(way, step, at):
        xs = pl.ds(0, NX) if step < 3 else pl.ds(0 if way == 0 else NX // 2, NX // 2)
        origin = lax.rem(z + (NZ - step - at if way == 0 else step + at), NZ)
        ref = wall.at[origin, xs, pl.ds(0, half), :]
        return (ref, ref)

    def b_whole(from_z, from_x, part):
        return wall.at[from_z, from_x, pl.ds(half + part.start, part.size), :]

    def c_whole(from_z, from_x, part):
        return down.at[from_z, from_x, part, :]

    def o_half(way):
        return pl.ds(way * (width // 2), width // 2)

    def o_block(way, step, at):
        return (osend.at[1, o_half(way), :], orelay.at[way])

    def lr_block(way, step, at):
        return (lsend.at[1], lrelay.at[way])

    def m_block(way, step, at):
        part = o_half(way if step == 1 else 1 - way)
        return (osend.at[2 * way, part, :], orecv.at[way, part, :])

    kring = Ring(z_target, k_block, k_sems.at[0], k_sems.at[1], (4, 3))
    vring = Ring(z_target, v_block, v_sems.at[0], v_sems.at[1], (3, 4))
    qring = Ring(x_target, q_block, q_sems.at[0], q_sems.at[1], (2, 2))
    axring = Ring(x_target, ax_block, ax_sems.at[0], ax_sems.at[1], (2, 2))
    azring = Ring(z_target, az_block, az_sems.at[0], az_sems.at[1], (4, 4))
    oring = Ring(x_target, o_block, or_sems.at[0], or_sems.at[1], (1, 1))
    lring = Ring(x_target, lr_block, lr_sems.at[0], lr_sems.at[1], (1, 1))
    mring = Ring(x_target, m_block, o_sems.at[0], o_sems.at[1], (2, 2))
    later = Gather(
        half, b_whole, z, x, z_target, x_target, bz_sems, b1_sems, b2_sems
    )
    lowest = Gather(wide, c_whole, z, x, z_target, x_target, cz_sems, c1_sems, c2_sems)

    def x_peer(g, src, dst, sems):
        return pltpu.make_async_remote_copy(
            src_ref=src,
            dst_ref=dst,
            send_sem=sems.at[0, g - 1],
            recv_sem=sems.at[1, g - 1],
            device_id={"sp_1": lax.rem(x + g, NX)},
            device_id_type=MESH,
        )

    def l_copy(g):
        return x_peer(g, lsend.at[g - 1], lrecv.at[g - 1], l_sems)

    locals_ = [
        pltpu.make_async_copy(src, dst, local_sems.at[i])
        for i, (src, dst) in enumerate(
            (
                (q_ref, qb.at[0]),
                (k_ref, kb.at[0]),
                (v_ref, vb.at[0]),
                (wg_ref, gate_own),
                (wu_ref, up_own),
                (wd_ref, down.at[z, x]),
                (res_ref.at[pl.ds(pl.multiple_of(t * own, own), own), :], res),
                (wout_ref, wout),
            )
        )
    ]
    for copy in locals_:
        copy.start()
    barrier = pltpu.get_barrier_semaphore()
    greeted = [{"sp_0": lax.rem(z + s, NZ)} for s in (1, NZ - 1)]
    greeted += [{"sp_1": lax.rem(x + s, NX)} for s in range(1, NX)]
    greeted += [{"tp": lax.rem(t + s, NT)} for s in range(1, NT)]
    for device in greeted:
        pl.semaphore_signal(barrier, inc=1, device_id=device, device_id_type=MESH)
    high[...] = jnp.full_like(high, LOWEST)
    acc[...] = jnp.zeros_like(acc)
    for copy in locals_[:6]:
        copy.wait()
    wall[z, x] = jnp.concatenate([gate_own[...], up_own[...]], axis=1)
    spread_queries(qb[0], q2, 0)
    pl.semaphore_wait(barrier, len(greeted))

    qring.start(0)
    kring.start(0)
    vring.start(0)
    axring.start(0)
    later.along_z(0)

    def group_tile(g):
        cols = pl.ds(g * columns, columns)
        attend_tile(q2[cols, :], kb[0], vb[0], high.at[:, cols], acc.at[:, cols])

    def kv_step(s):
        kring.arrived(s)
        vring.arrived(s)
        if s < 3:
            kring.start(s + 1)
            vring.start(s + 1)

    def a_step(s):
        azring.arrived(s)
        if s < 3:
            azring.start(s + 1)

    group_tile(0)
    qring.arrived(0)
    qring.start(1)
    later.both_ways(0)
    kv_step(0)
    axring.arrived(0)
    axring.start(1)
    for g in (1, 3):
        spread_queries(qb[g], q2, g * columns)
        group_tile(g)
    qring.arrived(1)
    spread_queries(qb[2], q2, 2 * columns)
    group_tile(2)

    def weight_step(gather, k):
        gather.along_z(k)
        gather.both_ways(k)

    events = {
        1: [lambda: weight_step(later, 1), lambda: later.forward(0)],
        2: [lambda: kv_step(1)],
        3: [lambda: weight_step(later, 2), lambda: later.forward(1), lambda: weight_step(lowest, 0)],
        4: [lambda: kv_step(2), lambda: axring.arrived(1), lambda: azring.start(0)],
    }

    def tile(i, carry):
        for at, todo in events.items():

            @pl.when(i == at)
            def _():
                for act in todo:
                    act()

        attend_tile(q2[...], kb[i], vb[i], high, acc)
        return carry

    lax.fori_loop(1, SPLIT, tile, 0)

    def last_tile(g):
        cols = pl.ds(g * columns, columns)
        keys = kb[SPLIT:].reshape(-1, kb.shape[-1])
        values = vb[SPLIT:].reshape(-1, vb.shape[-1])
        attend_tile(q2[cols, :], keys, values, high.at[:, cols], acc.at[:, cols])

    def result(g):
        cols = pl.ds(g * columns, columns)
        totals = acc[pl.ds(width, 1), cols]
        return acc[pl.ds(0, width), cols] / totals, high[:, cols] + jnp.log(totals)

    def stored(g):
        mix, lse = result(g)
        osend[g - 1] = mix.astype(osend.dtype)
        lsend[g - 1] = jnp.broadcast_to(lse, lsend.shape[1:])

    weight_step(later, 3)
    later.forward(2)
    kv_step(3)
    def joined(way):
        g = 1 if way == 0 else 3
        mix, lse = result(g)
        first = way * (width // 2)
        mix = mix[first : first + width // 2]
        other = lrelay[way][:1]
        top = jnp.maximum(lse, other)
        here, there = jnp.exp(lse - top), jnp.exp(other - top)
        mix = (mix * here + orelay[way].astype(jnp.float32) * there) / (here + there)
        osend[g - 1, first : first + width // 2] = mix.astype(osend.dtype)

    last_tile(2)
    stored(2)
    oring.start(0)
    lring.start(0)
    l_copy(2).start()
    last_tile(1)
    stored(1)
    mring.copy(0, 0, 0).start()
    l_copy(1).start()
    lowest.along_z(1)
    last_tile(3)
    stored(3)
    mring.copy(1, 0, 0).start()
    l_copy(3).start()
    a_step(0)
    oring.arrived(0)
    lring.arrived(0)
    joined(0)
    joined(1)
    mring.start(1)
    lowest.along_z(2)
    last_tile(0)
    mix, lse = result(0)
    later.along_z(4)
    later.both_ways(4)
    later.forward(3)
    lowest.both_ways(1)
    lowest.forward(0)
    mring.arrived(0)
    mring.arrived(1)
    for g in range(1, NX):
        l_copy(g).wait_recv()
    lses = [lse] + [lrecv[g][:1] for g in range(NX - 1)]
    top = functools.reduce(jnp.maximum, lses)
    mine, left, far, right = [jnp.exp(one - top) for one in lses]
    from_left, from_right = orecv[0].astype(jnp.float32), orecv[1].astype(jnp.float32)
    mix = jnp.concatenate(
        [
            mix[: width // 2] * mine
            + from_left[: width // 2] * (left + far)
            + from_right[: width // 2] * right,
            mix[width // 2 :] * mine
            + from_left[width // 2 :] * left
            + from_right[width // 2 :] * (right + far),
        ],
        axis=0,
    )
    mix = mix / (mine + left + far + right)
    differ = mix[:, :rows] - lam_ref[0] * mix[:, rows:]
    square = jnp.mean(differ * differ, axis=0, keepdims=True)
    mine = (differ * lax.rsqrt(square + 1e-05)).T * gain_ref[...]
    heads[...] = mine.astype(heads.dtype)

    def own_rows(index):
        return pl.ds(pl.multiple_of(index * own, own), own)

    def h_copy(d, to, home):
        return pltpu.make_async_remote_copy(
            src_ref=heads.at[own_rows(to), :],
            dst_ref=th.at[home],
            send_sem=h_sems.at[0, d - 1],
            recv_sem=h_sems.at[1, d - 1],
            device_id={"tp": to},
            device_id_type=MESH,
        )

    for d in range(1, NT):
        h_copy(d, lax.rem(t + d, NT), t).start()
    th[t] = heads[own_rows(t), :]
    a_step(1)
    lowest.along_z(3)
    later.forward(4)
    lowest.both_ways(2)
    lowest.both_ways(3)
    for copy in locals_[6:]:
        copy.wait()
    for d in range(1, NT):
        h_copy(d, lax.rem(t + d, NT), lax.rem(t + NT - d, NT)).wait_recv()
    token_heads = jnp.concatenate([th[h] for h in range(NT)], axis=1)
    projected = jnp.dot(token_heads, wout[...], preferred_element_type=jnp.float32)
    stream = (res[...].astype(jnp.float32) + projected).astype(jnp.bfloat16)
    hidden[...] = stream
    stream = stream.astype(jnp.float32)
    scale = lax.rsqrt(jnp.mean(stream * stream, axis=-1, keepdims=True) + 1e-05)
    normed[t] = (stream * scale * norm_gain_ref[...]).astype(normed.dtype)

    def y_block(way, step, at):
        part = pl.ds((1 - way if step == 1 else way) * (own // 2), own // 2)
        hops = step // 2 + at
        ref = normed.at[chip(NY - hops if way == 0 else hops) * 2 + core, part, :]
        return (ref, ref)

    yring = Ring(y_target, y_block, y_sems.at[0], y_sems.at[1], (3, 3))
    shared = ((0, 0, own), (NY - 1, 0, own), (1, 0, own), (2, 0, own // 2), (2, own // 2, own // 2))

    def p_copy(number, of_core):
        offset, first, count = shared[number]
        ref = normed.at[chip(offset) * 2 + of_core, pl.ds(first, count), :]
        return pltpu.make_async_remote_copy(
            src_ref=ref,
            dst_ref=ref,
            send_sem=p_sems.at[0, number],
            recv_sem=p_sems.at[1, number],
            device_id=partner,
            device_id_type=MESH,
        )

    yring.start(0)
    yring.start(1)
    p_copy(0, core).start()
    yring.arrived(0)
    yring.start(2)
    a_step(2)
    weight_step(lowest, 4)
    lowest.forward(1)
    yring.arrived(1)
    p_copy(1, core).start()
    p_copy(2, core).start()
    lowest.forward(2)
    yring.arrived(2)
    p_copy(3, core).start()
    p_copy(4, core).start()
    lowest.forward(3)
    later.done()
    azring.arrived(3)
    lowest.forward(4)
    for number in range(len(shared)):
        p_copy(number, 1 - core).wait_recv()
    inputs = normed[...].reshape(rows, -1)
    both = wall[...].reshape(-1, wall.shape[-1])
    sums = jnp.dot(inputs, both, preferred_element_type=jnp.float32)
    gate, up = sums[:, :unit_width], sums[:, unit_width:]
    gated = gate / (1.0 + jnp.exp(-gate)) * up
    units[...] = gated.astype(units.dtype).reshape(units.shape)
    lowest.done()

    def piece(offsets):
        lhs = jnp.concatenate([units[pl.ds(chip(o) * 2, 2)] for o in offsets], axis=0)
        part = lax.dot_general(
            lhs.reshape(-1, unit_width),
            down[...].reshape(-1, unit_width),
            (((1,), (1,)), ((), ())),
            preferred_element_type=jnp.float32,
        )
        part = part.reshape(len(offsets), *parts.shape[1:])
        for i, o in enumerate(offsets):
            parts[o] = part[i]
            pb[o] = parts[o, 1 - core].astype(pb.dtype)

    def pair_copy(offset):
        return pltpu.make_async_remote_copy(
            src_ref=pb.at[offset],
            dst_ref=pr.at[offset],
            send_sem=c_sems.at[0, offset],
            recv_sem=c_sems.at[1, offset],
            device_id=partner,
            device_id_type=MESH,
        )

    def paired(offset):
        pair_copy(offset).wait_recv()
        return parts[offset, core] + pr[offset].astype(jnp.float32)

    def r_block(way, step, at):
        part = pl.ds((way if step == 1 else 1 - way) * (own // 2), own // 2)
        return (fs.at[1 if way == 0 else NY - 1, part, :], fr.at[way, part, :])

    def rr_block(way, step, at):
        return (fs.at[2, pl.ds(way * (own // 2), own // 2), :], relay.at[way])

    rring = Ring(y_target, r_block, r_sems.at[0], r_sems.at[1], (2, 2))
    rrring = Ring(y_target, rr_block, rr_sems.at[0], rr_sems.at[1], (1, 1))
    piece((2, 3))
    pair_copy(2).start()
    pair_copy(3).start()
    piece((1, 0))
    pair_copy(1).start()
    pair_copy(0).start()
    fs[2] = paired(2).astype(fs.dtype)
    rrring.start(0)
    ahead = paired(1)
    fs[1, own // 2 :] = ahead[own // 2 :].astype(fs.dtype)
    behind = paired(3)
    fs[3, : own // 2] = behind[: own // 2].astype(fs.dtype)
    rring.start(0)
    total = hidden[...].astype(jnp.float32) + paired(0)
    rrring.arrived(0)
    fs[1, : own // 2] = (ahead[: own // 2] + relay[0].astype(jnp.float32)).astype(fs.dtype)
    fs[3, own // 2 :] = (behind[own // 2 :] + relay[1].astype(jnp.float32)).astype(fs.dtype)
    rring.start(1)
    rring.arrived(0)
    rring.arrived(1)
    total = total + fr[0].astype(jnp.float32) + fr[1].astype(jnp.float32)
    out_ref[...] = total.astype(out_ref.dtype)

    for ring in (kring, vring, qring, axring, azring, oring, lring, mring, later, lowest, yring, rring, rrring):
        ring.sent()
    for g in range(1, NX):
        l_copy(g).wait_send()
    for d in range(1, NT):
        h_copy(d, lax.rem(t + d, NT), t).wait_send()
    for number in range(len(shared)):
        p_copy(number, core).wait_send()
    for offset in range(NY):
        pair_copy(offset).wait_send()


def layer(q, k, v, wg, wu, wd, lambdas, gain, norm_gain, residual, w_out):
    rows, width = v.shape
    model = residual.shape[1]
    columns = NX * 2 * rows
    own = rows // NT
    wide, units = wg.shape
    vmem = pl.BlockSpec(memory_space=pltpu.VMEM)
    smem = pl.BlockSpec(memory_space=pltpu.SMEM)
    hbm = pl.BlockSpec(memory_space=pl.ANY)
    dma = pltpu.SemaphoreType.DMA
    short, long = jnp.bfloat16, jnp.float32
    return pl.pallas_call(
        layer_kernel,
        out_shape=jax.ShapeDtypeStruct((own, model), short),
        in_specs=[hbm] * 6 + [smem, vmem, vmem, hbm, hbm],
        out_specs=vmem,
        scratch_shapes=[
            pltpu.VMEM((NX, rows, 2 * HD), short),
            pltpu.VMEM((NZ, rows, 2 * HD), short),
            pltpu.VMEM((NZ, rows, width), short),
            pltpu.VMEM((columns, 2 * HD), short),
            pltpu.VMEM((1, columns), long),
            pltpu.VMEM((width + EXTRA, columns), long),
            pltpu.VMEM((NX - 1, width, 2 * rows), short),
            pltpu.VMEM((NX - 1, 8, 2 * rows), long),
            pltpu.VMEM((2, width, 2 * rows), short),
            pltpu.VMEM((NX - 1, 8, 2 * rows), long),
            pltpu.VMEM((2, width // 2, 2 * rows), short),
            pltpu.VMEM((NZ, NX, wide, 2 * units), short),
            pltpu.VMEM((NZ, NX, *wd.shape), short),
            pltpu.VMEM(w_out.shape, short),
            pltpu.VMEM((own, model), short),
            pltpu.VMEM((rows, width), short),
            pltpu.VMEM((NT, own, width), short),
            pltpu.VMEM((NT, own, model), short),
            pltpu.VMEM((own, model), short),
            pltpu.VMEM((NT, own, units), short),
            pltpu.VMEM((NY, 2, own, model), long),
            pltpu.VMEM((NY, own, model), short),
            pltpu.VMEM((NY, own, model), short),
            pltpu.VMEM((NY, own, model), short),
            pltpu.VMEM((2, own, model), short),
            pltpu.VMEM((2, own // 2, model), short),
            dma((2, 2, 2)),
            dma((2, 2, 4)),
            dma((2, 2, 4)),
            dma((2, 2, 2)),
            dma((2, 2, 4)),
            dma((2, 2, 4)),
            dma((2, 2, NZ)),
            dma((2, 2, NZ)),
            dma((2, 2, 4)),
            dma((2, 2, NZ)),
            dma((2, 2, NZ)),
            dma((2, 2, 2)),
            dma((2, NX - 1)),
            dma((2, 2, 1)),
            dma((8,)),
            dma((2, NT - 1)),
            dma((2, 2, 3)),
            dma((2, 5)),
            dma((2, NY)),
            dma((2, 2, 2)),
            dma((2, 2, 1)),
            pltpu.VMEM((wide, units), short),
            pltpu.VMEM((wide, units), short),
            pltpu.VMEM((2, 8, 2 * rows), long),
            dma((2, 2, 1)),
        ],
        compiler_params=pltpu.CompilerParams(
            vmem_limit_bytes=63 * 2**20, collective_id=0, has_side_effects=True
        ),
    )(q, k, v, wg, wu, wd, lambdas, gain, norm_gain, residual, w_out)


def per_device(
    residual, queries, key_pairs, values, lambdas, head_gain, w_out, norm_gain, w_gate, w_up, w_down
):
    return layer(
        queries,
        key_pairs,
        values,
        w_gate,
        w_up,
        w_down.T,
        lambdas,
        head_gain[None, :],
        norm_gain[None, :],
        residual,
        w_out,
    )


def solution(mesh):
    torus = Mesh(mesh.devices.reshape(NZ, NX, NT), ("sp_0", "sp_1", "tp"))
    return jax.shard_map(
        per_device,
        mesh=torus,
        in_specs=(
            P(SP, None),
            P(SP, "tp"),
            P(SP, "tp"),
            P(SP, "tp"),
            P("tp"),
            P(),
            P(),
            P(),
            P(SP, "tp"),
            P(SP, "tp"),
            P("tp", SP),
        ),
        out_specs=P(SP_TP, None),
        check_vma=False,
    )
```

```python
import functools

import jax
import jax.numpy as jnp
from jax import lax
from jax.experimental import pallas as pl
from jax.experimental.pallas import tpu as pltpu
from jax.sharding import Mesh
from jax.sharding import PartitionSpec as P

HD = 64
SP = ("sp_0", "sp_1")
SP_TP = ("sp_0", "sp_1", "tp")
LOWEST = -1e30
EXTRA = 16
SPLIT = 5
NZ = 8
NX = 4
NY = 4
NT = 8
MESH = pl.DeviceIdType.MESH


def spread_queries(q, out_ref, at):
    rows = q.shape[0]
    lane = lax.broadcasted_iota(jnp.int32, q.shape, 1)
    zero = jnp.zeros_like(q)
    q = q * jnp.asarray(HD**-0.5, q.dtype)
    out_ref[pl.ds(at, rows), :] = jnp.where(lane < HD, q, zero)
    out_ref[pl.ds(at + rows, rows), :] = jnp.where(lane >= HD, q, zero)


def attend_tile(q2, keys, values, high_ref, acc_ref):
    one_row = lax.broadcasted_iota(jnp.int32, (EXTRA, keys.shape[0]), 0) == 0
    ones = jnp.where(one_row, 1.0, 0.0).astype(values.dtype)
    values_t = jnp.concatenate([values.T, ones], axis=0)
    scores = lax.dot_general(
        keys, q2, (((1,), (1,)), ((), ())), preferred_element_type=jnp.float32
    )
    before = high_ref[...]
    after = jnp.maximum(before, jnp.max(scores, axis=0, keepdims=True))
    shrink = jnp.exp(before - after)
    weights = jnp.exp(scores - after).astype(jnp.bfloat16)
    mixed = jnp.dot(values_t, weights, preferred_element_type=jnp.float32)
    acc_ref[...] = acc_ref[...] * shrink + mixed
    high_ref[...] = after


class Ring:
    def __init__(self, target, block, send, recv, steps):
        self.target, self.block = target, block
        self.send, self.recv, self.steps = send, recv, steps

    def copy(self, way, step, at):
        src, dst = self.block(way, step, at)
        return pltpu.make_async_remote_copy(
            src_ref=src,
            dst_ref=dst,
            send_sem=self.send.at[way, step],
            recv_sem=self.recv.at[way, step],
            device_id=self.target(way),
            device_id_type=MESH,
        )

    def start(self, step):
        for way in (0, 1):
            if step < self.steps[way]:
                self.copy(way, step, 0).start()

    def arrived(self, step):
        for way in (0, 1):
            if step < self.steps[way]:
                self.copy(way, step, 1).wait_recv()

    def sent(self):
        for way in (0, 1):
            for step in range(self.steps[way]):
                self.copy(way, step, 0).wait_send()


class Gather:
    def __init__(self, rows, whole, z, x, z_target, x_target, z_sems, one_sems, two_sems):
        self.rows, self.whole, self.z, self.x = rows, whole, z, x
        self.x_target, self.one, self.two = x_target, one_sems, two_sems
        self.ring = Ring(z_target, self.z_block, z_sems.at[0], z_sems.at[1], (4, 4))

    def origin(self, index):
        step = (index + 1) // 2
        return lax.rem(self.z + (NZ - step if index % 2 else step), NZ)

    def z_block(self, way, step, at):
        half = self.rows // 2
        rows = pl.ds(0, self.rows) if step < 3 else pl.ds(half * way, half)
        origin = lax.rem(self.z + (NZ - step - at if way == 0 else step + at), NZ)
        ref = self.whole(origin, self.x, rows)
        return (ref, ref)

    def along_x(self, src, dst, sems, way, index):
        return pltpu.make_async_remote_copy(
            src_ref=src,
            dst_ref=dst,
            send_sem=sems.at[0, way, index],
            recv_sem=sems.at[1, way, index],
            device_id=self.x_target(way),
            device_id_type=MESH,
        )

    def hop(self, number, way, index, at):
        step = number - 1 + at
        from_x = lax.rem(self.x + (NX - step if way == 0 else step), NX)
        ref = self.whole(self.origin(index), from_x, pl.ds(0, self.rows))
        return self.along_x(ref, ref, self.one if number == 1 else self.two, way, index)

    def members(self, k):
        return [0] if k == 0 else [7] if k == 4 else [2 * k - 1, 2 * k]

    def second_way(self, index):
        return 0 if index in (0, 1, 3, 5) else 1

    def along_z(self, k):
        if k > 0:
            self.ring.arrived(k - 1)
        if k < 4:
            self.ring.start(k)

    def both_ways(self, k):
        for index in self.members(k):
            for way in (0, 1):
                self.hop(1, way, index, 0).start()

    def forward(self, k):
        for index in self.members(k):
            for way in (0, 1):
                self.hop(1, way, index, 1).wait_recv()
            self.hop(2, self.second_way(index), index, 0).start()

    def done(self):
        for index in range(NZ):
            self.hop(2, self.second_way(index), index, 1).wait_recv()

    def sent(self):
        self.ring.sent()
        for index in range(NZ):
            for way in (0, 1):
                self.hop(1, way, index, 0).wait_send()
            self.hop(2, self.second_way(index), index, 0).wait_send()


def layer_kernel(
    q_ref, k_ref, v_ref, wg_ref, wu_ref, wd_ref, lam_ref, gain_ref, norm_gain_ref, res_ref, wout_ref,
    out_ref,
    qb, kb, vb, q2, high, acc, osend, lsend, orecv, lrecv, orelay,
    wall, down, wout, res, heads, th, normed, hidden, units, parts, pb, pr, fs, fr, relay,
    q_sems, k_sems, v_sems, ax_sems, az_sems, bz_sems, b1_sems, b2_sems,
    cz_sems, c1_sems, c2_sems, o_sems, l_sems, or_sems, local_sems,
    h_sems, y_sems, p_sems, c_sems, r_sems, rr_sems, gate_own, up_own,
    lrelay, lr_sems,
):
    z, x, t = lax.axis_index("sp_0"), lax.axis_index("sp_1"), lax.axis_index("tp")
    y, core = t // 2, lax.rem(t, 2)
    rows, width = vb.shape[1:]
    wide, unit_width = wg_ref.shape
    half = wide // 2
    columns = 2 * rows
    own = rows // NT

    def z_target(way):
        return {"sp_0": lax.rem(z + (1 if way == 0 else NZ - 1), NZ)}

    def x_target(way):
        return {"sp_1": lax.rem(x + (1 if way == 0 else NX - 1), NX)}

    def chip(offset):
        return lax.rem(y + offset, NY)

    def y_target(way):
        return {"tp": chip(1 if way == 0 else NY - 1) * 2 + core}

    partner = {"tp": t + 1 - 2 * core}

    def slot(way, step):
        return 0 if step == 0 else 2 * step - 1 if way == 0 else 7 if step == 4 else 2 * step

    def k_block(way, step, at):
        return (kb.at[slot(way, step + at)], kb.at[slot(way, step + 1)])

    def v_block(way, step, at):
        return (vb.at[slot(way, step + at)], vb.at[slot(way, step + 1)])

    def q_block(way, step, at):
        part = pl.ds(0, rows) if step == 0 else pl.ds(way * (rows // 2), rows // 2)
        place = lambda hops: (NX - hops if way == 0 else hops) % NX
        return (qb.at[place(step + at), part, :], qb.at[place(step + 1), part, :])

    def ax_block(way, step, at):
        part = pl.ds(0, half) if step == 0 else pl.ds(way * (half // 2), half // 2)
        from_x = lax.rem(x + (NX - step - at if way == 0 else step + at), NX)
        ref = wall.at[z, from_x, part, :]
        return (ref, ref)

    def az_block(way, step, at):
        xs = pl.ds(0, NX) if step < 3 else pl.ds(0 if way == 0 else NX // 2, NX // 2)
        origin = lax.rem(z + (NZ - step - at if way == 0 else step + at), NZ)
        ref = wall.at[origin, xs, pl.ds(0, half), :]
        return (ref, ref)

    def b_whole(from_z, from_x, part):
        return wall.at[from_z, from_x, pl.ds(half + part.start, part.size), :]

    def c_whole(from_z, from_x, part):
        return down.at[from_z, from_x, part, :]

    def o_half(way):
        return pl.ds(way * (width // 2), width // 2)

    def o_block(way, step, at):
        return (osend.at[1, o_half(way), :], orelay.at[way])

    def lr_block(way, step, at):
        return (lsend.at[1], lrelay.at[way])

    def m_block(way, step, at):
        part = o_half(way if step == 1 else 1 - way)
        return (osend.at[2 * way, part, :], orecv.at[way, part, :])

    kring = Ring(z_target, k_block, k_sems.at[0], k_sems.at[1], (4, 3))
    vring = Ring(z_target, v_block, v_sems.at[0], v_sems.at[1], (3, 4))
    qring = Ring(x_target, q_block, q_sems.at[0], q_sems.at[1], (2, 2))
    axring = Ring(x_target, ax_block, ax_sems.at[0], ax_sems.at[1], (2, 2))
    azring = Ring(z_target, az_block, az_sems.at[0], az_sems.at[1], (4, 4))
    oring = Ring(x_target, o_block, or_sems.at[0], or_sems.at[1], (1, 1))
    lring = Ring(x_target, lr_block, lr_sems.at[0], lr_sems.at[1], (1, 1))
    mring = Ring(x_target, m_block, o_sems.at[0], o_sems.at[1], (2, 2))
    later = Gather(
        half, b_whole, z, x, z_target, x_target, bz_sems, b1_sems, b2_sems
    )
    lowest = Gather(wide, c_whole, z, x, z_target, x_target, cz_sems, c1_sems, c2_sems)

    def x_peer(g, src, dst, sems):
        return pltpu.make_async_remote_copy(
            src_ref=src,
            dst_ref=dst,
            send_sem=sems.at[0, g - 1],
            recv_sem=sems.at[1, g - 1],
            device_id={"sp_1": lax.rem(x + g, NX)},
            device_id_type=MESH,
        )

    def l_copy(g):
        return x_peer(g, lsend.at[g - 1], lrecv.at[g - 1], l_sems)

    locals_ = [
        pltpu.make_async_copy(src, dst, local_sems.at[i])
        for i, (src, dst) in enumerate(
            (
                (q_ref, qb.at[0]),
                (k_ref, kb.at[0]),
                (v_ref, vb.at[0]),
                (wg_ref, gate_own),
                (wu_ref, up_own),
                (wd_ref, down.at[z, x]),
                (res_ref.at[pl.ds(pl.multiple_of(t * own, own), own), :], res),
                (wout_ref, wout),
            )
        )
    ]
    for copy in locals_:
        copy.start()
    barrier = pltpu.get_barrier_semaphore()
    greeted = [{"sp_0": lax.rem(z + s, NZ)} for s in (1, NZ - 1)]
    greeted += [{"sp_1": lax.rem(x + s, NX)} for s in range(1, NX)]
    greeted += [{"tp": lax.rem(t + s, NT)} for s in range(1, NT)]
    for device in greeted:
        pl.semaphore_signal(barrier, inc=1, device_id=device, device_id_type=MESH)
    high[...] = jnp.full_like(high, LOWEST)
    acc[...] = jnp.zeros_like(acc)
    for copy in locals_[:6]:
        copy.wait()
    wall[z, x] = jnp.concatenate([gate_own[...], up_own[...]], axis=1)
    spread_queries(qb[0], q2, 0)
    pl.semaphore_wait(barrier, len(greeted))

    qring.start(0)
    kring.start(0)
    vring.start(0)
    axring.start(0)
    later.along_z(0)

    def group_tile(g):
        cols = pl.ds(g * columns, columns)
        attend_tile(q2[cols, :], kb[0], vb[0], high.at[:, cols], acc.at[:, cols])

    def kv_step(s):
        kring.arrived(s)
        vring.arrived(s)
        if s < 3:
            kring.start(s + 1)
            vring.start(s + 1)

    def a_step(s):
        azring.arrived(s)
        if s < 3:
            azring.start(s + 1)

    group_tile(0)
    qring.arrived(0)
    qring.start(1)
    later.both_ways(0)
    kv_step(0)
    lowest.both_ways(0)
    axring.arrived(0)
    axring.start(1)
    for g in (1, 3):
        spread_queries(qb[g], q2, g * columns)
        group_tile(g)
    qring.arrived(1)
    spread_queries(qb[2], q2, 2 * columns)
    group_tile(2)

    def weight_step(gather, k):
        gather.along_z(k)
        gather.both_ways(k)

    events = {
        1: [lambda: weight_step(later, 1), lambda: later.forward(0)],
        2: [lambda: kv_step(1)],
        3: [lambda: weight_step(later, 2), lambda: later.forward(1), lambda: lowest.along_z(0)],
        4: [
            lambda: kv_step(2),
            lambda: axring.arrived(1),
            lambda: azring.start(0),
            lambda: lowest.forward(0),
        ],
    }

    def tile(i, carry):
        for at, todo in events.items():

            @pl.when(i == at)
            def _():
                for act in todo:
                    act()

        attend_tile(q2[...], kb[i], vb[i], high, acc)
        return carry

    lax.fori_loop(1, SPLIT, tile, 0)

    def last_tile(g):
        cols = pl.ds(g * columns, columns)
        keys = kb[SPLIT:].reshape(-1, kb.shape[-1])
        values = vb[SPLIT:].reshape(-1, vb.shape[-1])
        attend_tile(q2[cols, :], keys, values, high.at[:, cols], acc.at[:, cols])

    def result(g):
        cols = pl.ds(g * columns, columns)
        totals = acc[pl.ds(width, 1), cols]
        return acc[pl.ds(0, width), cols] / totals, high[:, cols] + jnp.log(totals)

    def stored(g):
        mix, lse = result(g)
        osend[g - 1] = mix.astype(osend.dtype)
        lsend[g - 1] = jnp.broadcast_to(lse, lsend.shape[1:])

    weight_step(later, 3)
    later.forward(2)
    kv_step(3)
    def joined(way):
        g = 1 if way == 0 else 3
        mix, lse = result(g)
        first = way * (width // 2)
        mix = mix[first : first + width // 2]
        other = lrelay[way][:1]
        top = jnp.maximum(lse, other)
        here, there = jnp.exp(lse - top), jnp.exp(other - top)
        mix = (mix * here + orelay[way].astype(jnp.float32) * there) / (here + there)
        osend[g - 1, first : first + width // 2] = mix.astype(osend.dtype)

    last_tile(2)
    stored(2)
    oring.start(0)
    lring.start(0)
    l_copy(2).start()
    last_tile(1)
    stored(1)
    mring.copy(0, 0, 0).start()
    l_copy(1).start()
    lowest.along_z(1)
    last_tile(3)
    stored(3)
    mring.copy(1, 0, 0).start()
    l_copy(3).start()
    a_step(0)
    oring.arrived(0)
    lring.arrived(0)
    joined(0)
    joined(1)
    mring.start(1)
    lowest.along_z(2)
    last_tile(0)
    mix, lse = result(0)
    later.along_z(4)
    later.both_ways(4)
    later.forward(3)
    lowest.both_ways(1)
    mring.arrived(0)
    mring.arrived(1)
    for g in range(1, NX):
        l_copy(g).wait_recv()
    lses = [lse] + [lrecv[g][:1] for g in range(NX - 1)]
    top = functools.reduce(jnp.maximum, lses)
    mine, left, far, right = [jnp.exp(one - top) for one in lses]
    from_left, from_right = orecv[0].astype(jnp.float32), orecv[1].astype(jnp.float32)
    mix = jnp.concatenate(
        [
            mix[: width // 2] * mine
            + from_left[: width // 2] * (left + far)
            + from_right[: width // 2] * right,
            mix[width // 2 :] * mine
            + from_left[width // 2 :] * left
            + from_right[width // 2 :] * (right + far),
        ],
        axis=0,
    )
    mix = mix / (mine + left + far + right)
    differ = mix[:, :rows] - lam_ref[0] * mix[:, rows:]
    square = jnp.mean(differ * differ, axis=0, keepdims=True)
    mine = (differ * lax.rsqrt(square + 1e-05)).T * gain_ref[...]
    heads[...] = mine.astype(heads.dtype)

    def own_rows(index):
        return pl.ds(pl.multiple_of(index * own, own), own)

    def h_copy(d, to, home):
        return pltpu.make_async_remote_copy(
            src_ref=heads.at[own_rows(to), :],
            dst_ref=th.at[home],
            send_sem=h_sems.at[0, d - 1],
            recv_sem=h_sems.at[1, d - 1],
            device_id={"tp": to},
            device_id_type=MESH,
        )

    for d in range(1, NT):
        h_copy(d, lax.rem(t + d, NT), t).start()
    th[t] = heads[own_rows(t), :]
    a_step(1)
    lowest.along_z(3)
    later.forward(4)
    lowest.both_ways(2)
    lowest.both_ways(3)
    for copy in locals_[6:]:
        copy.wait()
    for d in range(1, NT):
        h_copy(d, lax.rem(t + d, NT), lax.rem(t + NT - d, NT)).wait_recv()
    token_heads = jnp.concatenate([th[h] for h in range(NT)], axis=1)
    projected = jnp.dot(token_heads, wout[...], preferred_element_type=jnp.float32)
    stream = (res[...].astype(jnp.float32) + projected).astype(jnp.bfloat16)
    hidden[...] = stream
    stream = stream.astype(jnp.float32)
    scale = lax.rsqrt(jnp.mean(stream * stream, axis=-1, keepdims=True) + 1e-05)
    normed[t] = (stream * scale * norm_gain_ref[...]).astype(normed.dtype)

    def y_block(way, step, at):
        part = pl.ds((1 - way if step == 1 else way) * (own // 2), own // 2)
        hops = step // 2 + at
        ref = normed.at[chip(NY - hops if way == 0 else hops) * 2 + core, part, :]
        return (ref, ref)

    yring = Ring(y_target, y_block, y_sems.at[0], y_sems.at[1], (3, 3))
    shared = ((0, 0, own), (NY - 1, 0, own), (1, 0, own), (2, 0, own // 2), (2, own // 2, own // 2))

    def p_copy(number, of_core):
        offset, first, count = shared[number]
        ref = normed.at[chip(offset) * 2 + of_core, pl.ds(first, count), :]
        return pltpu.make_async_remote_copy(
            src_ref=ref,
            dst_ref=ref,
            send_sem=p_sems.at[0, number],
            recv_sem=p_sems.at[1, number],
            device_id=partner,
            device_id_type=MESH,
        )

    yring.start(0)
    yring.start(1)
    p_copy(0, core).start()
    yring.arrived(0)
    yring.start(2)
    a_step(2)
    weight_step(lowest, 4)
    lowest.forward(1)
    yring.arrived(1)
    p_copy(1, core).start()
    p_copy(2, core).start()
    lowest.forward(2)
    yring.arrived(2)
    p_copy(3, core).start()
    p_copy(4, core).start()
    lowest.forward(3)
    later.done()
    azring.arrived(3)
    lowest.forward(4)
    for number in range(len(shared)):
        p_copy(number, 1 - core).wait_recv()
    inputs = normed[...].reshape(rows, -1)
    both = wall[...].reshape(-1, wall.shape[-1])
    sums = jnp.dot(inputs, both, preferred_element_type=jnp.float32)
    gate, up = sums[:, :unit_width], sums[:, unit_width:]
    gated = gate / (1.0 + jnp.exp(-gate)) * up
    units[...] = gated.astype(units.dtype).reshape(units.shape)
    lowest.done()

    def piece(offsets):
        lhs = jnp.concatenate([units[pl.ds(chip(o) * 2, 2)] for o in offsets], axis=0)
        part = lax.dot_general(
            lhs.reshape(-1, unit_width),
            down[...].reshape(-1, unit_width),
            (((1,), (1,)), ((), ())),
            preferred_element_type=jnp.float32,
        )
        part = part.reshape(len(offsets), *parts.shape[1:])
        for i, o in enumerate(offsets):
            parts[o] = part[i]
            pb[o] = parts[o, 1 - core].astype(pb.dtype)

    def pair_copy(offset):
        return pltpu.make_async_remote_copy(
            src_ref=pb.at[offset],
            dst_ref=pr.at[offset],
            send_sem=c_sems.at[0, offset],
            recv_sem=c_sems.at[1, offset],
            device_id=partner,
            device_id_type=MESH,
        )

    def paired(offset):
        pair_copy(offset).wait_recv()
        return parts[offset, core] + pr[offset].astype(jnp.float32)

    def r_block(way, step, at):
        part = pl.ds((way if step == 1 else 1 - way) * (own // 2), own // 2)
        return (fs.at[1 if way == 0 else NY - 1, part, :], fr.at[way, part, :])

    def rr_block(way, step, at):
        return (fs.at[2, pl.ds(way * (own // 2), own // 2), :], relay.at[way])

    rring = Ring(y_target, r_block, r_sems.at[0], r_sems.at[1], (2, 2))
    rrring = Ring(y_target, rr_block, rr_sems.at[0], rr_sems.at[1], (1, 1))
    piece((2, 3))
    pair_copy(2).start()
    pair_copy(3).start()
    piece((1, 0))
    pair_copy(1).start()
    pair_copy(0).start()
    fs[2] = paired(2).astype(fs.dtype)
    rrring.start(0)
    ahead = paired(1)
    fs[1, own // 2 :] = ahead[own // 2 :].astype(fs.dtype)
    behind = paired(3)
    fs[3, : own // 2] = behind[: own // 2].astype(fs.dtype)
    rring.start(0)
    total = hidden[...].astype(jnp.float32) + paired(0)
    rrring.arrived(0)
    fs[1, : own // 2] = (ahead[: own // 2] + relay[0].astype(jnp.float32)).astype(fs.dtype)
    fs[3, own // 2 :] = (behind[own // 2 :] + relay[1].astype(jnp.float32)).astype(fs.dtype)
    rring.start(1)
    rring.arrived(0)
    rring.arrived(1)
    total = total + fr[0].astype(jnp.float32) + fr[1].astype(jnp.float32)
    out_ref[...] = total.astype(out_ref.dtype)

    for ring in (kring, vring, qring, axring, azring, oring, lring, mring, later, lowest, yring, rring, rrring):
        ring.sent()
    for g in range(1, NX):
        l_copy(g).wait_send()
    for d in range(1, NT):
        h_copy(d, lax.rem(t + d, NT), t).wait_send()
    for number in range(len(shared)):
        p_copy(number, core).wait_send()
    for offset in range(NY):
        pair_copy(offset).wait_send()


def layer(q, k, v, wg, wu, wd, lambdas, gain, norm_gain, residual, w_out):
    rows, width = v.shape
    model = residual.shape[1]
    columns = NX * 2 * rows
    own = rows // NT
    wide, units = wg.shape
    vmem = pl.BlockSpec(memory_space=pltpu.VMEM)
    smem = pl.BlockSpec(memory_space=pltpu.SMEM)
    hbm = pl.BlockSpec(memory_space=pl.ANY)
    dma = pltpu.SemaphoreType.DMA
    short, long = jnp.bfloat16, jnp.float32
    return pl.pallas_call(
        layer_kernel,
        out_shape=jax.ShapeDtypeStruct((own, model), short),
        in_specs=[hbm] * 6 + [smem, vmem, vmem, hbm, hbm],
        out_specs=vmem,
        scratch_shapes=[
            pltpu.VMEM((NX, rows, 2 * HD), short),
            pltpu.VMEM((NZ, rows, 2 * HD), short),
            pltpu.VMEM((NZ, rows, width), short),
            pltpu.VMEM((columns, 2 * HD), short),
            pltpu.VMEM((1, columns), long),
            pltpu.VMEM((width + EXTRA, columns), long),
            pltpu.VMEM((NX - 1, width, 2 * rows), short),
            pltpu.VMEM((NX - 1, 8, 2 * rows), long),
            pltpu.VMEM((2, width, 2 * rows), short),
            pltpu.VMEM((NX - 1, 8, 2 * rows), long),
            pltpu.VMEM((2, width // 2, 2 * rows), short),
            pltpu.VMEM((NZ, NX, wide, 2 * units), short),
            pltpu.VMEM((NZ, NX, *wd.shape), short),
            pltpu.VMEM(w_out.shape, short),
            pltpu.VMEM((own, model), short),
            pltpu.VMEM((rows, width), short),
            pltpu.VMEM((NT, own, width), short),
            pltpu.VMEM((NT, own, model), short),
            pltpu.VMEM((own, model), short),
            pltpu.VMEM((NT, own, units), short),
            pltpu.VMEM((NY, 2, own, model), long),
            pltpu.VMEM((NY, own, model), short),
            pltpu.VMEM((NY, own, model), short),
            pltpu.VMEM((NY, own, model), short),
            pltpu.VMEM((2, own, model), short),
            pltpu.VMEM((2, own // 2, model), short),
            dma((2, 2, 2)),
            dma((2, 2, 4)),
            dma((2, 2, 4)),
            dma((2, 2, 2)),
            dma((2, 2, 4)),
            dma((2, 2, 4)),
            dma((2, 2, NZ)),
            dma((2, 2, NZ)),
            dma((2, 2, 4)),
            dma((2, 2, NZ)),
            dma((2, 2, NZ)),
            dma((2, 2, 2)),
            dma((2, NX - 1)),
            dma((2, 2, 1)),
            dma((8,)),
            dma((2, NT - 1)),
            dma((2, 2, 3)),
            dma((2, 5)),
            dma((2, NY)),
            dma((2, 2, 2)),
            dma((2, 2, 1)),
            pltpu.VMEM((wide, units), short),
            pltpu.VMEM((wide, units), short),
            pltpu.VMEM((2, 8, 2 * rows), long),
            dma((2, 2, 1)),
        ],
        compiler_params=pltpu.CompilerParams(
            vmem_limit_bytes=63 * 2**20, collective_id=0, has_side_effects=True
        ),
    )(q, k, v, wg, wu, wd, lambdas, gain, norm_gain, residual, w_out)


def per_device(
    residual, queries, key_pairs, values, lambdas, head_gain, w_out, norm_gain, w_gate, w_up, w_down
):
    return layer(
        queries,
        key_pairs,
        values,
        w_gate,
        w_up,
        w_down.T,
        lambdas,
        head_gain[None, :],
        norm_gain[None, :],
        residual,
        w_out,
    )


def solution(mesh):
    torus = Mesh(mesh.devices.reshape(NZ, NX, NT), ("sp_0", "sp_1", "tp"))
    return jax.shard_map(
        per_device,
        mesh=torus,
        in_specs=(
            P(SP, None),
            P(SP, "tp"),
            P(SP, "tp"),
            P(SP, "tp"),
            P("tp"),
            P(),
            P(),
            P(),
            P(SP, "tp"),
            P(SP, "tp"),
            P("tp", SP),
        ),
        out_specs=P(SP_TP, None),
        check_vma=False,
    )
```
